256 devices in a mesh: gr: 2 (over z_hi), fs: 16 (over z_lo, y), tp: 8 (over x, core).
Axes of the slice: x: 4, y: 4, z: 8 (z_hi: 2, z_lo: 4; z = z_hi * 4 + z_lo), core: 2. Of those that a mesh axis runs over, the one named last changes fastest.
Arguments:
- tokens: bfloat16 [8192, 2048], P(('gr', 'tp'), 'fs'), may hold values from -6 to 6
- routes: int32 [8192, 2], P(('gr', 'tp')), may hold values from 0 to 7, all different within a row; in each aligned block of 512 rows (0 to 511, 512 to 1023, ...) at most 192 rows name the same one
- route_weight: float32 [8192, 2], P(('gr', 'tp')), may hold values from 0.25 to 1
- norm_gain: float32 [2048], P(('gr', 'fs')), may hold values from 0.1 to 1.9
- gate_master: float32 [8, 2048, 2816], P(None, ('gr', 'fs'), 'tp'), may hold values from -0.125 to 0.125
- up_master: float32 [8, 2048, 2816], P(None, ('gr', 'fs'), 'tp'), may hold values from -0.125 to 0.125
- down_master: float32 [8, 2048, 2816], P(None, ('gr', 'fs'), 'tp'), may hold values from -0.109375 to 0.109375
Outputs:
- mixed_output: bfloat16 [8192, 2048], P(('gr', 'tp'), 'fs')
- gate_serving: bfloat16 [8, 2048, 2816], P('tp', None, 'fs')
- up_serving: bfloat16 [8, 2048, 2816], P('tp', None, 'fs')
- down_serving: bfloat16 [8, 2048, 2816], P('tp', None, 'fs')
The draws below stay inside these ranges and needn't reach their ends.
Inputs may be any that keep to these rules, and one draw needn't show every extreme that they name: `routes`: each row names two different experts. Within the rows of one block of 512 tokens (one index of gr+tp) no expert is named by more than 192 rows, and in some blocks one expert is named by exactly 192.
All inputs are finite; a program needn't handle non-finite values.
Results may differ from the reference program's by a relative error of at most 0.0082.
Values may be sent and summed in bfloat16 or wider, within the bound.
A program may use at most 128 MiB of HBM per device.

```python
import math
import jax
import jax.numpy as jnp
import numpy as np
from jax import lax

D = 2048
EFF = 2816
EXPERTS = 8
TOK_DEV = 512
CAP = 192
TOKENS = 8192


def shard_levels(stream_key, dims, cuts, low, largest):
    loudness, own = 1.0, jax.random.fold_in(stream_key, 6)
    for dim, blocks in cuts:
        steps = jnp.exp(jax.random.uniform(jax.random.fold_in(own, dim), (blocks,), jnp.float32, low / len(cuts), largest / len(cuts)))
        loudness = loudness * jnp.repeat(steps, dims[dim] // blocks).reshape([-1 if axis == dim else 1 for axis in range(len(dims))])
    return loudness


def deal_out(stream_key, own, number, rows, count, top, bound, skew):
    ranking = jax.random.permutation(stream_key, count)
    heavy_load, common = portions_of(count, rows * top, bound, skew, True), portions_of(count, rows * top, bound, skew, False)
    places = jnp.arange(count)

    def named(tallies, rotation):
        used = int((tallies > 0).sum())
        fixed = max(1, used // 4)
        passed = fixed + (places - fixed + rotation * (used - fixed)) % max(1, count - fixed)
        return jnp.zeros((count,), jnp.int32).at[ranking[jnp.where(places < fixed, places, passed)]].set(jnp.asarray(tallies, jnp.int32))

    tallies = jnp.where(number % 4 == 0, named(heavy_load, number // 4), named(common, number - number // 4 - 1))
    mixed = jax.random.permutation(jax.random.fold_in(own, 3), count)
    source_of, sink = mixed[0:count // 2 * 2:2], mixed[1:count // 2 * 2:2]
    slack = jnp.minimum(tallies[source_of] - 1, bound - tallies[sink]) // 2
    slack = jnp.where((source_of == ranking[0]) | (sink == ranking[0]) | (tallies[sink] == 0), 0, jnp.maximum(slack, 0))
    passed = jax.random.randint(jax.random.fold_in(own, 4), (count // 2,), 0, 1 << 20) % (slack + 1)
    tallies = tallies.at[source_of].add(-passed).at[sink].add(passed)
    members = jnp.searchsorted(jnp.cumsum(tallies), jnp.arange(rows * top), side="right").astype(jnp.int32)
    grid = members.reshape(top, rows).T
    grid = grid[jax.random.permutation(jax.random.fold_in(own, 1), rows)]
    rotation = jax.random.randint(jax.random.fold_in(own, 2), (rows, 1), 0, top)
    return jnp.take_along_axis(grid, (jnp.arange(top)[None, :] + rotation) % top, axis=1)


def portions_of(count, total, reach, slope, full):
    portions = [(1 << 20) // math.isqrt(standing ** slope) + 1 for standing in range(1, count + 1)]
    largest = reach if full else min(reach, max(-(-total // count), total * portions[0] // sum(portions)))
    least = 1 if total - largest >= count - 1 else 0
    holding, rest = [largest] + [least] * (count - 1), total - largest - least * (count - 1)
    while rest > 0:
        candidates = [i for i in range(1, count) if holding[i] < largest] or [i for i in range(1, count) if holding[i] < reach]
        whole, left = sum([portions[i] for i in candidates]), rest
        for i in candidates:
            addition = min(reach - holding[i], max(1, left * portions[i] // whole), rest)
            holding[i] = holding[i] + addition
            rest = rest - addition
    return np.array(holding)


def normal_values(key, shape, deviation, bound, cuts=(), held_as=jnp.bfloat16):
    values = deviation * jax.random.normal(key, shape, jnp.float32)
    if cuts:
        values = values * shard_levels(key, shape, cuts, -0.22, 0.18)
    return jnp.clip(values, -bound, bound).astype(held_as)


def setup_inputs(seed: int = 0) -> dict:
    arg_keys = jax.random.split(jax.random.key(seed), 8)
    tokens = normal_values(arg_keys[0], (TOKENS, D), 1.0, 6.0, ((0, 16), (1, 16)))
    routes_keys = jax.random.split(jax.random.fold_in(arg_keys[1], 1), TOKENS // TOK_DEV)
    routes_turns = jax.random.permutation(jax.random.fold_in(arg_keys[1], 3), TOKENS // TOK_DEV)
    routes = jax.vmap(lambda own, number: deal_out(jax.random.fold_in(arg_keys[1], 2), own, number, TOK_DEV, EXPERTS, 2, CAP, 1))(routes_keys, routes_turns).reshape((TOKENS, 2))
    route_weight = jnp.clip(jnp.exp(math.log(1.0) - 1.3862944 * jax.random.uniform(arg_keys[2], (TOKENS, 2), jnp.float32) ** shard_levels(arg_keys[2], (TOKENS, 2), ((0, 16),), -0.2, 0.2)), 0.25, 1.0)
    norm_gain = jnp.clip(1.0 + 0.18 * jax.random.normal(arg_keys[3], (D,), jnp.float32), 0.1, 1.9)
    gate_master = normal_values(arg_keys[4], (EXPERTS, D, EFF), D ** -0.5, 0.125, ((1, 32), (2, 8)), jnp.float32)
    up_master = normal_values(arg_keys[5], (EXPERTS, D, EFF), D ** -0.5, 0.125, ((1, 32), (2, 8)), jnp.float32)
    down_master = normal_values(arg_keys[6], (EXPERTS, D, EFF), EFF ** -0.5, 0.109375, ((1, 32), (2, 8)), jnp.float32)
    return {"tokens": tokens, "routes": routes, "route_weight": route_weight, "norm_gain": norm_gain, "gate_master": gate_master, "up_master": up_master, "down_master": down_master}


norm_eps = 1e-06

def slot_table(routes, experts, capacity):
    flat_routes = routes.reshape(-1)
    onehot = (flat_routes[:, None] == jnp.arange(experts, dtype=jnp.int32)[None, :]).astype(jnp.int32)
    running = jnp.cumsum(onehot, axis=0)
    slot_index = lax.optimization_barrier(jnp.sum(onehot * (running - 1), axis=1))
    return (flat_routes * capacity + slot_index).astype(jnp.int32)

def reference(tokens, routes, route_weight, norm_gain, gate_master, up_master, down_master):
    gate_serving = (gate_master * norm_gain[None, :, None]).astype(jnp.bfloat16)
    up_serving = (up_master * norm_gain[None, :, None]).astype(jnp.bfloat16)
    down_serving = down_master.astype(jnp.bfloat16)
    blocks = TOKENS // TOK_DEV
    as_float = tokens.astype(jnp.float32)
    normed = (as_float * lax.rsqrt(lax.optimization_barrier(jnp.mean(as_float * as_float, axis=1, keepdims=True)) + norm_eps)).astype(jnp.bfloat16)
    normed = normed.reshape(blocks, TOK_DEV, D)
    route_blocks = routes.reshape(blocks, TOK_DEV, 2)

    def find_slots(block_routes):
        return slot_table(block_routes, EXPERTS, CAP)
    placing = jax.vmap(find_slots)(route_blocks)
    slot_rows = jnp.arange(EXPERTS * CAP, dtype=jnp.int32)

    def pick(block_places):
        return (slot_rows[:, None] == block_places[None, :]).reshape(EXPERTS * CAP, TOK_DEV, 2)

    def dispatch(block_places, block_rows):
        route_table = lax.optimization_barrier(jnp.sum(pick(block_places).astype(jnp.float32), axis=2)).astype(jnp.bfloat16)
        return jnp.dot(route_table, block_rows, preferred_element_type=jnp.float32).astype(jnp.bfloat16)
    outgoing = jax.vmap(dispatch)(placing, normed)
    outgoing = outgoing.reshape(blocks, EXPERTS, CAP, D).transpose(1, 0, 2, 3).reshape(EXPERTS, blocks * CAP, D)

    def expert(inputs):
        slots, w_gate, w_up, w_down = inputs
        gate_acc = jnp.dot(slots, w_gate, preferred_element_type=jnp.float32)
        up_acc = jnp.dot(slots, w_up, preferred_element_type=jnp.float32)
        hidden = (jax.nn.silu(gate_acc) * up_acc).astype(jnp.bfloat16)
        return lax.dot_general(hidden, w_down, (((1,), (1,)), ((), ())), preferred_element_type=jnp.float32)
    outputs = lax.map(expert, (outgoing, gate_serving, up_serving, down_serving))
    outputs = outputs.reshape(EXPERTS, blocks, CAP, D).transpose(1, 0, 2, 3).reshape(blocks, EXPERTS * CAP, D)

    def combine(block_places, weight, produced):
        weights = lax.optimization_barrier(jnp.sum(jnp.where(pick(block_places), weight.reshape(1, TOK_DEV, 2), 0.0), axis=2))
        return lax.dot_general(weights, produced, (((0,), (0,)), ((), ())), precision=lax.Precision.HIGHEST, preferred_element_type=jnp.float32)
    mixed_output = jax.vmap(combine)(placing, route_weight.reshape(blocks, TOK_DEV, 2), outputs)
    return (mixed_output.reshape(TOKENS, D).astype(jnp.bfloat16), gate_serving, up_serving, down_serving)
```

```python
import jax
import jax.numpy as jnp
from jax import lax
from jax.experimental import pallas as pl
from jax.experimental.pallas import tpu as pltpu
from jax.sharding import PartitionSpec as P

norm_eps = 1e-06
BF = jnp.bfloat16
F32 = jnp.float32
I32 = jnp.int32
MESH = pl.DeviceIdType.MESH
VMEM_LIMIT = 60 * 1024 * 1024

NY, NZ, NX, NC = 4, 4, 4, 2
NT = NX * NC
EXPERTS = 8
CAP = 192
ROWS = 64
COLS = 176
LANES = 128
TAIL = COLS - LANES
PACK = 3 * ROWS + ROWS + 16
TOK = 512
FEAT = 128
ZF = NZ * FEAT
KS = (4, 3, 5, 2, 6, 1, 7, 0)


def coords():
    g, f, t = lax.axis_index("gr"), lax.axis_index("fs"), lax.axis_index("tp")
    return g, lax.div(f, NY), lax.rem(f, NY), t


def at(g, z, y, t):
    return (g, z * NY + y, t)


def rem(a, n):
    return lax.rem(a, n)


def send(src, dst, ss, rs, to):
    return pltpu.make_async_remote_copy(
        src_ref=src, dst_ref=dst, send_sem=ss, recv_sem=rs, device_id=to, device_id_type=MESH
    )


def slot_keys(routes_ref):
    ex = lax.broadcasted_iota(I32, (16, TOK), 0)
    named = (routes_ref[0:1, :] == ex) | (routes_ref[1:2, :] == ex)
    ones = jnp.where(named, 1.0, 0.0).astype(BF)
    before = lax.broadcasted_iota(I32, (TOK, TOK), 0) < lax.broadcasted_iota(I32, (TOK, TOK), 1)
    rank = jnp.dot(ones, jnp.where(before, 1.0, 0.0).astype(BF), preferred_element_type=F32)
    return jnp.where(named, rank, -1.0)


def gather_kernel(
    tok_ref, routes_ref, gain_ref, gm_ref, um_ref, dm_ref,
    v_ref, x_ref,
    key_ref, wp_ref, q_ref, t_ref, s_ref,
    zs, zr, qs, qr, vs, vr, xs, xr, ys, yr,
):
    g, z, y, t = coords()
    x, c = lax.div(t, NC), lax.rem(t, NC)
    up_y, dn_y = rem(y + 1, NY), rem(y + NY - 1, NY)

    barrier = pltpu.get_barrier_semaphore()
    count = 0
    for dy in range(NY):
        for dt in range(NT):
            if dy or dt:
                pl.semaphore_signal(barrier, inc=1, device_id=at(g, z, rem(y + dy, NY), rem(t + dt, NT)), device_id_type=MESH)
                count += 1
    for dg in range(2):
        for dz in range(NZ):
            if dg or dz:
                pl.semaphore_signal(barrier, inc=1, device_id=at(rem(g + dg, 2), rem(z + dz, NZ), y, t), device_id_type=MESH)
                count += 1

    gain = gain_ref[...]
    for k in KS:
        e = rem(t + k, NT)
        gw, uw, dw = gm_ref[e] * gain, um_ref[e] * gain, dm_ref[e]
        for h in range(2):
            lo = h * COLS
            for j, w in enumerate((gw, uw, dw)):
                wp_ref[k, h, j * ROWS:(j + 1) * ROWS, :] = w[:, lo:lo + LANES].astype(BF)
            gt, ut, dt_ = (w[:, lo + LANES:lo + COLS] for w in (gw, uw, dw))
            wp_ref[k, h, 3 * ROWS:4 * ROWS, :] = jnp.concatenate([gt, ut, dt_[:, :32]], axis=1).astype(BF)
            rest = dt_[:, 32:48]
            extra = jnp.concatenate([rest[8 * i:8 * i + 8] for i in range(8)], axis=1)
            wp_ref[k, h, 4 * ROWS:4 * ROWS + 16, :] = jnp.concatenate([extra, jnp.zeros_like(extra)], axis=0).astype(BF)
    key_ref[...] = slot_keys(routes_ref)

    pl.semaphore_wait(barrier, count)

    tok_sends = []
    for j in (3, 2, 1):
        d = send(tok_ref, t_ref.at[z], zs.at[j], zr.at[j], at(g, rem(z + j, NZ), y, t))
        d.start()
        tok_sends.append(d)
    own_tok = pltpu.make_async_copy(tok_ref, t_ref.at[z], zr.at[0])
    own_tok.start()

    def first(k, h):
        return send(
            wp_ref.at[k, h], q_ref.at[x, y], qs.at[k, h], qr.at[x * NY + y],
            at(g, z, NC * c + h, rem(t + k, NT)),
        )

    def first_own(h):
        return pltpu.make_async_copy(wp_ref.at[0, h], q_ref.at[x, y], qr.at[x * NY + y])

    for k in KS:
        for h in range(2):
            if k:
                first(k, h).start()
            else:
                mine = NC * c + h == y

                @pl.when(mine)
                def _():
                    first_own(h).start()

                @pl.when(jnp.logical_not(mine))
                def _():
                    first(k, h).start()

    own_tok.wait()
    for j in (1, 2, 3):
        tok_sends[3 - j].wait_recv()
    rows_in = jnp.concatenate([t_ref[i] for i in range(NZ)], axis=1)
    slot = lax.broadcasted_iota(I32, (CAP, TOK), 0).astype(F32)
    for k in KS:
        key = key_ref[pl.ds(rem(t + k, NT), 1), :]
        table = jnp.where(slot == key, 1.0, 0.0).astype(BF)
        s_ref[k] = jnp.dot(table, rows_in, preferred_element_type=F32).astype(BF)

    def across(k):
        return send(s_ref.at[k], x_ref.at[t, y], xs.at[k], xr.at[k], at(g, z, y, rem(t + k, NT)))

    own_rows = pltpu.make_async_copy(s_ref.at[0], x_ref.at[t, y], xr.at[0])
    own_rows.start()
    for k in KS[:-1]:
        across(k).start()

    zz = g * NZ + z

    def second(j, q):
        zd = rem(z + j, NZ)
        return send(q_ref.at[zd], v_ref.at[zz], vs.at[j, q], vr.at[j, q], at(rem(g + q, 2), zd, y, t))

    own_v = pltpu.make_async_copy(q_ref.at[z], v_ref.at[zz], vr.at[0, 0])
    for j in (2, 1, 3, 0):
        zd = rem(z + j, NZ)
        for i in range(NY):
            send(wp_ref.at[0, 0], q_ref.at[zd, i], qs.at[0, 0], qr.at[zd * NY + i], at(g, z, up_y, t)).wait_recv()
        for q in (1, 0):
            if j or q:
                second(j, q).start()
            else:
                own_v.start()

    def block(k):
        return rem(t + NT - k, NT)

    def along(k, way):
        b = block(k)
        if way == 0:
            return send(x_ref.at[b, y], x_ref.at[b, y], ys.at[k, 0], yr.at[k, 0], at(g, z, up_y, t))
        if way == 1:
            return send(x_ref.at[b, y], x_ref.at[b, y], ys.at[k, 1], yr.at[k, 1], at(g, z, dn_y, t))
        if k % 2 == 0:
            return send(x_ref.at[b, dn_y], x_ref.at[b, dn_y], ys.at[k, 2], yr.at[k, 2], at(g, z, up_y, t))
        return send(x_ref.at[b, up_y], x_ref.at[b, up_y], ys.at[k, 2], yr.at[k, 2], at(g, z, dn_y, t))

    order = (0, 1, 7, 2, 6, 3, 5, 4)
    for i, k in enumerate(order):
        if k:
            across(k).wait_recv()
        else:
            own_rows.wait()
        along(k, 0).start()
        along(k, 1).start()
        if i >= 2:
            p = order[i - 2]
            along(p, p % 2).wait_recv()
            along(p, 2).start()
    for p in order[-2:]:
        along(p, p % 2).wait_recv()
        along(p, 2).start()

    for k in order:
        along(k, 1 - k % 2).wait_recv()
        along(k, 2).wait_recv()
        for way in range(3):
            along(k, way).wait_send()
        if k:
            across(k).wait_send()
    own_v.wait()
    for j in range(NZ):
        for q in range(2):
            if j or q:
                second(j, q).wait()
    for d in tok_sends:
        d.wait_send()
    for k in KS:
        for h in range(2):
            if k:
                first(k, h).wait_send()
            else:
                @pl.when(NC * c + h != y)
                def _():
                    first(k, h).wait_send()


def expert_kernel(v_ref, x_ref, gate_ref, up_ref, down_ref, p_ref):
    @pl.when(pl.program_id(0) == 0)
    def _():
        lane = lax.broadcasted_iota(I32, (ROWS, LANES), 1)

        def piece(i, _):
            zi, yi = lax.div(i, NY), lax.rem(i, NY)
            rows = pl.ds(pl.multiple_of(i * ROWS, ROWS), ROWS)
            for j, w in enumerate((gate_ref, up_ref, down_ref)):
                w[0, rows, 0:LANES] = v_ref[zi, yi, j * ROWS:(j + 1) * ROWS, :]
            tails = v_ref[zi, yi, 3 * ROWS:4 * ROWS, :].astype(F32)
            extra = v_ref[zi, yi, 4 * ROWS:4 * ROWS + 16, :].astype(F32)[0:8]
            rest = jnp.concatenate([pltpu.roll(extra, (32 + LANES - 16 * n) % LANES, 1) for n in range(8)], axis=0)
            gate_ref[0, rows, LANES:COLS] = tails[:, 0:TAIL].astype(BF)
            up_ref[0, rows, LANES:COLS] = pltpu.roll(tails, LANES - TAIL, 1)[:, 0:TAIL].astype(BF)
            down_tail = jnp.where(lane < 32, pltpu.roll(tails, LANES - 2 * TAIL, 1), rest)
            down_ref[0, rows, LANES:COLS] = down_tail[:, 0:TAIL].astype(BF)
            return 0

        lax.fori_loop(0, 2 * NZ * NY, piece, 0)

    rows = jnp.concatenate(
        [x_ref[0, yi, :, zi * FEAT:(zi + 1) * FEAT] for zi in range(NZ) for yi in range(NY)], axis=1
    )
    wide = rows.astype(F32)
    scale = lax.rsqrt(jnp.sum(wide * wide, axis=1, keepdims=True) / (NZ * NY * FEAT) + norm_eps)
    gate = jnp.dot(rows, gate_ref[0], preferred_element_type=F32) * scale
    up = jnp.dot(rows, up_ref[0], preferred_element_type=F32) * scale
    hidden = (gate / (1.0 + jnp.exp(-gate)) * up).astype(BF)
    out = lax.dot_general(hidden, down_ref[0], (((1,), (1,)), ((), ())), preferred_element_type=F32).astype(BF)
    for zi in range(NZ):
        for yi in range(NY):
            f = zi * NY + yi
            p_ref[0, yi, :, zi * FEAT:(zi + 1) * FEAT] = out[:, f * FEAT:(f + 1) * FEAT]


def reduce_kernel(
    p_ref, routes_ref, weight_ref,
    out_ref,
    key_ref, mix_ref, r_ref, a_ref, u_ref, w_ref, o_ref, e_ref, m_ref, l_ref,
    rs, rr, us, ur, ws, wr, os, orr, zs, zr,
):
    g, z, y, t = coords()
    up_y, dn_y, far_y = rem(y + 1, NY), rem(y + NY - 1, NY), rem(y + 2, NY)

    barrier = pltpu.get_barrier_semaphore()
    count = 0
    for to in (
        [at(g, z, up_y, t), at(g, z, dn_y, t)]
        + [at(g, z, y, rem(t + k, NT)) for k in range(1, NT)]
        + [at(g, rem(z + j, NZ), y, t) for j in range(1, NZ)]
    ):
        pl.semaphore_signal(barrier, inc=1, device_id=to, device_id_type=MESH)
        count += 1

    keys = slot_keys(routes_ref)
    key_ref[...] = keys
    ex = lax.broadcasted_iota(I32, (16, TOK), 0)
    mix_ref[...] = jnp.where(routes_ref[0:1, :] == ex, weight_ref[0:1, :], 0.0) + jnp.where(
        routes_ref[1:2, :] == ex, weight_ref[1:2, :], 0.0
    )
    pl.semaphore_wait(barrier, count)

    def block(k):
        return rem(t + k, NT)

    def near(k):
        return up_y if k % 2 == 0 else dn_y

    def other(k):
        return dn_y if k % 2 == 0 else up_y

    def far(k):
        return send(p_ref.at[block(k), far_y], r_ref.at[k], rs.at[k], rr.at[k], at(g, z, near(k), t))

    def plain(k):
        return send(p_ref.at[block(k), other(k)], u_ref.at[k], us.at[k], ur.at[k], at(g, z, other(k), t))

    def summed(k):
        return send(a_ref.at[k], w_ref.at[k], ws.at[k], wr.at[k], at(g, z, near(k), t))

    def back(k):
        return send(o_ref.at[k], e_ref.at[t], os.at[k], orr.at[k], at(g, z, y, block(k)))

    for k in KS:
        far(k).start()
    for k in KS:
        plain(k).start()

    def finish(k):
        plain(k).wait_recv()
        summed(k).wait_recv()
        total = p_ref[block(k), y].astype(F32) + u_ref[k].astype(F32) + w_ref[k].astype(F32)
        if k:
            o_ref[k] = total.astype(BF)
            back(k).start()
        else:
            e_ref[t] = total.astype(BF)

    for i, k in enumerate(KS):
        far(k).wait_recv()
        a_ref[k] = (r_ref[k].astype(F32) + p_ref[block(k), near(k)].astype(F32)).astype(BF)
        summed(k).start()
        if i >= 2:
            finish(KS[i - 2])
    for k in KS[-2:]:
        finish(k)

    slot = lax.broadcasted_iota(I32, (CAP, TOK), 0).astype(F32)
    total = jnp.zeros((TOK, ZF), F32)
    for k in (0, 4, 5, 3, 6, 2, 7, 1):
        e = rem(t + NT - k, NT)
        if k:
            back(k).wait_recv()
        key, mix = key_ref[pl.ds(e, 1), :], mix_ref[pl.ds(e, 1), :]
        mix_hi = mix.astype(BF).astype(F32)
        here = slot == key
        produced = e_ref[e]
        for part in (mix_hi, mix - mix_hi):
            table = jnp.where(here, part, 0.0).astype(BF)
            total = total + lax.dot_general(table, produced, (((0,), (0,)), ((), ())), preferred_element_type=F32)
    for i in range(NZ):
        m_ref[i] = total[:, i * FEAT:(i + 1) * FEAT].astype(BF)

    def part(j):
        zd = rem(z + j, NZ)
        return send(m_ref.at[zd], l_ref.at[j], zs.at[j], zr.at[j], at(g, zd, y, t))

    for j in (3, 2, 1):
        part(j).start()
    own = m_ref[z].astype(F32)
    for j in (1, 2, 3):
        part(j).wait_recv()
        own = own + l_ref[j].astype(F32)
    out_ref[...] = own.astype(BF)

    for k in KS:
        far(k).wait_send()
        plain(k).wait_send()
        summed(k).wait_send()
        if k:
            back(k).wait_send()
    for j in (1, 2, 3):
        part(j).wait_send()


def local(tokens, routes, route_weight, norm_gain, gate_master, up_master, down_master):
    vm = pl.BlockSpec(memory_space=pltpu.VMEM)
    any_ = pl.BlockSpec(memory_space=pl.ANY)
    dma = pltpu.SemaphoreType.DMA
    routes_t = routes.T
    weight_t = route_weight.T
    v, rows = pl.pallas_call(
        gather_kernel,
        out_shape=(
            jax.ShapeDtypeStruct((2 * NZ, NY, PACK, LANES), BF),
            jax.ShapeDtypeStruct((NT, NY, CAP, ZF), BF),
        ),
        in_specs=[vm] * 6,
        out_specs=(any_, any_),
        scratch_shapes=[
            pltpu.VMEM((16, TOK), F32),
            pltpu.VMEM((NT, 2, PACK, LANES), BF),
            pltpu.VMEM((NX, NY, PACK, LANES), BF),
            pltpu.VMEM((NZ, TOK, FEAT), BF),
            pltpu.VMEM((NT, CAP, ZF), BF),
            dma((NZ,)), dma((NZ,)),
            dma((NT, 2)), dma((NX * NY,)),
            dma((NZ, 2)), dma((NZ, 2)),
            dma((NT,)), dma((NT,)),
            dma((NT, 3)), dma((NT, 3)),
        ],
        compiler_params=pltpu.CompilerParams(collective_id=0, has_side_effects=True, vmem_limit_bytes=VMEM_LIMIT),
        name="gather_kernel",
    )(tokens, routes_t, norm_gain[:, None], gate_master, up_master, down_master)

    serving = jax.ShapeDtypeStruct((1, 2048, COLS), BF)
    whole = pl.BlockSpec((1, 2048, COLS), lambda b: (0, 0, 0))
    per_block = pl.BlockSpec((1, NY, CAP, ZF), lambda b: (b, 0, 0, 0))
    gate_w, up_w, down_w, partial = pl.pallas_call(
        expert_kernel,
        grid=(NT,),
        out_shape=(serving, serving, serving, jax.ShapeDtypeStruct((NT, NY, CAP, ZF), BF)),
        in_specs=[pl.BlockSpec((2 * NZ, NY, PACK, LANES), lambda b: (0, 0, 0, 0)), per_block],
        out_specs=(whole, whole, whole, per_block),
        compiler_params=pltpu.CompilerParams(vmem_limit_bytes=VMEM_LIMIT),
        name="expert_kernel",
    )(v, rows)

    buf = pltpu.VMEM((NT, CAP, ZF), BF)
    mixed = pl.pallas_call(
        reduce_kernel,
        out_shape=jax.ShapeDtypeStruct((TOK, FEAT), BF),
        in_specs=[vm] * 3,
        out_specs=vm,
        scratch_shapes=[
            pltpu.VMEM((16, TOK), F32),
            pltpu.VMEM((16, TOK), F32),
            buf, buf, buf, buf, buf, buf,
            pltpu.VMEM((NZ, TOK, FEAT), BF),
            pltpu.VMEM((NZ, TOK, FEAT), BF),
            dma((NT,)), dma((NT,)), dma((NT,)), dma((NT,)), dma((NT,)), dma((NT,)), dma((NT,)), dma((NT,)),
            dma((NZ,)), dma((NZ,)),
        ],
        compiler_params=pltpu.CompilerParams(collective_id=1, has_side_effects=True, vmem_limit_bytes=VMEM_LIMIT),
        name="reduce_kernel",
    )(partial, routes_t, weight_t)
    return mixed, gate_w, up_w, down_w


def solution(mesh):
    placed = (
        P(("gr", "tp"), "fs"),
        P(("gr", "tp"), None),
        P(("gr", "tp"), None),
        P(("gr", "fs")),
        P(None, ("gr", "fs"), "tp"),
        P(None, ("gr", "fs"), "tp"),
        P(None, ("gr", "fs"), "tp"),
    )
    return jax.shard_map(
        local,
        mesh=mesh,
        in_specs=placed,
        out_specs=(
            P(("gr", "tp"), "fs"),
            P("tp", None, "fs"),
            P("tp", None, "fs"),
            P("tp", None, "fs"),
        ),
        check_vma=False,
    )
```

```python
import jax
import jax.numpy as jnp
from jax import lax
from jax.experimental import pallas as pl
from jax.experimental.pallas import tpu as pltpu
from jax.sharding import PartitionSpec as P

norm_eps = 1e-06
BF = jnp.bfloat16
F32 = jnp.float32
I32 = jnp.int32
MESH = pl.DeviceIdType.MESH
VMEM_LIMIT = 60 * 1024 * 1024

NY, NZ, NX, NC = 4, 4, 4, 2
NT = NX * NC
EXPERTS = 8
CAP = 192
ROWS = 64
WIDTH = 352
COLS = 176
LANES = 128
DLO, DHI = 96, 80
PACK = COLS + DLO
TOK = 512
FEAT = 128
MODEL = 2048
NEAR = (0, 1, 7, 2, 6, 3, 5, 4)
FARS = (4, 3, 5, 2, 6, 1, 7, 0)
HALVES = ((0, 3), (1, 2))


def rem(a, n):
    return lax.rem(a, n)


def at(g, z, y, t):
    return (g, z * NY + y, t)


def send(src, dst, ss, rs, to):
    return pltpu.make_async_remote_copy(
        src_ref=src, dst_ref=dst, send_sem=ss, recv_sem=rs, device_id=to, device_id_type=MESH
    )


def kernel(
    tok_ref, routes_ref, weight_ref, gain_ref, gm_hbm, um_hbm, dm_hbm,
    out_ref, gate_out, up_out, down_out,
    gm_ref, um_ref, dm_ref, key_ref, mix_ref, table_ref, comb_ref,
    wp_ref, q_ref, v_ref, t_ref, s_ref, x_ref, gate_ref, up_ref, down_ref, h_ref,
    p_ref, r_ref, a_ref, u_ref, w_ref, o_ref, e_ref, m_ref, l_ref,
    ms, zs, zr, qs, qr, vs, vr, xs, xr, ys, yr,
    fs, fr, us, ur, ws, wr, bs, br, cs, cr, outs,
):
    g, f, t = lax.axis_index("gr"), lax.axis_index("fs"), lax.axis_index("tp")
    z, y = lax.div(f, NY), rem(f, NY)
    x, c = lax.div(t, NC), rem(t, NC)
    up_y, dn_y, far_y = rem(y + 1, NY), rem(y + NY - 1, NY), rem(y + 2, NY)

    masters = [
        pltpu.make_async_copy(src, dst, ms.at[i])
        for i, (src, dst) in enumerate(((gm_hbm, gm_ref), (um_hbm, um_ref), (dm_hbm, dm_ref)))
    ]
    for m in masters:
        m.start()

    barrier = pltpu.get_barrier_semaphore()
    count = 0
    for dy in range(NY):
        for dt in range(NT):
            if dy or dt:
                pl.semaphore_signal(barrier, inc=1, device_id=at(g, z, rem(y + dy, NY), rem(t + dt, NT)), device_id_type=MESH)
                count += 1
    for dg in range(2):
        for dz in range(NZ):
            if dg or dz:
                pl.semaphore_signal(barrier, inc=1, device_id=at(rem(g + dg, 2), rem(z + dz, NZ), y, t), device_id_type=MESH)
                count += 1

    ex = lax.broadcasted_iota(I32, (16, TOK), 0)
    first_is, second_is = routes_ref[0:1, :] == ex, routes_ref[1:2, :] == ex
    named = first_is | second_is
    before = lax.broadcasted_iota(I32, (TOK, TOK), 0) < lax.broadcasted_iota(I32, (TOK, TOK), 1)
    rank = jnp.dot(
        jnp.where(named, 1.0, 0.0).astype(BF), jnp.where(before, 1.0, 0.0).astype(BF), preferred_element_type=F32
    )
    key_ref[...] = jnp.where(named, rank, -1.0)
    mix_ref[...] = jnp.where(first_is, weight_ref[0:1, :], 0.0) + jnp.where(second_is, weight_ref[1:2, :], 0.0)
    slot = lax.broadcasted_iota(I32, (CAP, TOK), 0).astype(F32)

    def tables(k, _):
        key = key_ref[pl.ds(rem(t + k, NT), 1), :]
        table_ref[k] = jnp.where(slot == key, 1.0, 0.0).astype(BF)
        return 0

    lax.fori_loop(0, NT, tables, 0)
    t_ref[z] = tok_ref[...]

    pl.semaphore_wait(barrier, count)

    low, base = rem(z, 2), 2 * lax.div(z, 2)
    peers = {1: base + 1 - low, 2: 2 - base + low, 3: 3 - base - low}

    def tok_copy(i):
        return send(tok_ref, t_ref.at[z], zs.at[i], zr.at[i], at(g, peers[i], y, t))

    for i in (1, 2, 3):
        tok_copy(i).start()

    def first(k, h):
        return send(
            wp_ref.at[k, h], q_ref.at[x, y], qs.at[k, h], qr.at[x * NY + y],
            at(g, z, NC * c + h, rem(t + k, NT)),
        )

    def first_start(k):
        for h in range(2):
            mine = (NC * c + h == y) & (rem(t + k, NT) == t)

            @pl.when(mine)
            def _():
                pltpu.make_async_copy(wp_ref.at[k, h], q_ref.at[x, y], qr.at[x * NY + y]).start()

            @pl.when(jnp.logical_not(mine))
            def _():
                first(k, h).start()

    for m in masters:
        m.wait()
    gain = jnp.concatenate([gain_ref[...], gain_ref[...]], axis=1)

    def pack(i, _):
        k = 4 + (1 - 2 * rem(i, 2)) * lax.div(i + 1, 2)
        e = rem(t + k, NT)
        pad = jnp.zeros((2 * ROWS, 3 * LANES - WIDTH), F32)
        gu = jnp.concatenate([gm_ref[e], um_ref[e]], axis=0)
        gu = (jnp.transpose(jnp.concatenate([gu, pad], axis=1)) * gain).astype(BF)
        dn = dm_ref[e]
        dn = jnp.concatenate([dn, pad[:ROWS]], axis=1)
        dd = jnp.concatenate([dn, pltpu.roll(dn, 3 * LANES - DLO, 1)], axis=0)
        dd = jnp.transpose(dd).astype(BF)
        for h in range(2):
            lo = h * COLS
            wp_ref[k, h, 0:COLS, :] = gu[lo:lo + COLS]
            wp_ref[k, h, COLS:PACK, :] = dd[lo:lo + DLO]

        @pl.when(i > 0)
        def _():
            j = i - 1
            first_start(4 + (1 - 2 * rem(j, 2)) * lax.div(j + 1, 2))

        return 0

    lax.fori_loop(0, NT, pack, 0)
    first_start(0)

    def pair_of(q):
        return lax.div(z, 2) if q == 0 else 1 - lax.div(z, 2)

    def dispatch(q):
        lo = 2 * pair_of(q)
        rows_in = jnp.concatenate([t_ref[lo], t_ref[lo + 1]], axis=1)
        for k in NEAR:
            rows = jnp.dot(table_ref[k], rows_in, preferred_element_type=F32).astype(BF)
            if k:
                s_ref[q, k] = rows
            else:
                x_ref[pair_of(q), t, y] = rows

    def across(q, k):
        return send(s_ref.at[q, k], x_ref.at[pair_of(q), t, y], xs.at[q, k], xr.at[q, k], at(g, z, y, rem(t + k, NT)))

    def along(q, k, way):
        b = rem(t + NT - k, NT)
        whose = y if way < 2 else (dn_y if k % 2 == 0 else up_y)
        to = up_y if way == 0 or (way == 2 and k % 2 == 0) else dn_y
        ref = x_ref.at[pair_of(q), b, whose]
        return send(ref, ref, ys.at[q, k, way], yr.at[q, k, way], at(g, z, to, t))

    def spread(q, k):
        if k:
            across(q, k).wait_recv()
        along(q, k, 0).start()
        along(q, k, 1).start()

    def forward(q, k):
        along(q, k, k % 2).wait_recv()
        along(q, k, 2).start()

    zz = g * NZ + z

    def second(j, q):
        zd = rem(z + j, NZ)
        return send(q_ref.at[zd], v_ref.at[zz], vs.at[j, q], vr.at[j, q], at(rem(g + q, 2), zd, y, t))

    own_v = pltpu.make_async_copy(q_ref.at[z], v_ref.at[zz], vr.at[0, 0])

    def weights_on(j):
        zd = rem(z + j, NZ)
        for i in range(NY):
            send(q_ref.at[zd, i], q_ref.at[zd, i], qs.at[0, 0], qr.at[zd * NY + i], at(g, z, up_y, t)).wait_recv()
        for q in (1, 0):
            if j or q:
                second(j, q).start()
            else:
                own_v.start()

    tok_copy(1).wait_recv()
    dispatch(0)
    for k in NEAR[1:]:
        across(0, k).start()
    spread(0, 0)
    spread(0, 1)
    tok_copy(2).wait_recv()
    tok_copy(3).wait_recv()
    dispatch(1)
    for k in NEAR[1:]:
        across(1, k).start()
    spread(1, 0)
    spread(0, 7)
    for j in (2, 1, 3, 0):
        weights_on(j)
        spread(0, NEAR[3 + (2, 1, 3, 0).index(j)])
    spread(0, NEAR[7])
    for k in NEAR:
        forward(0, k)
        if k:
            spread(1, k)
    for k in NEAR:
        forward(1, k)

    def weighting(k, _):
        e = rem(t + NT - k, NT)
        here = slot == key_ref[pl.ds(e, 1), :]
        mix = mix_ref[pl.ds(e, 1), :]
        high = mix.astype(BF).astype(F32)
        for i, part in enumerate((high, mix - high)):
            comb_ref[k, i] = jnp.transpose(jnp.where(here, part, 0.0)).astype(BF)
        return 0

    lax.fori_loop(0, NT, weighting, 0)

    left = lax.broadcasted_iota(I32, (COLS, LANES), 1) < ROWS

    def unpack(zs_):
        for i in range(NY // 2):
            a, b = (v_ref[zs_, 2 * i + n].astype(F32) for n in range(2))
            ra, rb = pltpu.roll(a, ROWS, 1), pltpu.roll(b, ROWS, 1)
            cols = pl.ds(pl.multiple_of((zs_ * (NY // 2) + i) * LANES, LANES), LANES)
            gate_ref[:, cols] = jnp.where(left, a[:COLS], rb[:COLS]).astype(BF)
            up_ref[:, cols] = jnp.where(left, ra[:COLS], b[:COLS]).astype(BF)
            down_ref[0:DLO, cols] = jnp.where(left[:DLO], a[COLS:], rb[COLS:]).astype(BF)
            down_ref[DLO:COLS, cols] = jnp.where(left[:DHI], ra[COLS:COLS + DHI], b[COLS:COLS + DHI]).astype(BF)

    own_v.wait()
    unpack(zz)
    for j, q in ((1, 0), (3, 0), (2, 0), (1, 1), (3, 1), (2, 1), (0, 1)):
        second(j, q).wait_recv()
        unpack(rem(g + q, 2) * NZ + rem(z + NZ - j, NZ))
    served = [
        pltpu.make_async_copy(src, dst.at[0], outs.at[i])
        for i, (src, dst) in enumerate(((gate_ref, gate_out), (up_ref, up_out), (down_ref, down_out)))
    ]
    for m in served:
        m.start()

    for q in range(2):
        for k in NEAR:
            along(q, k, 1 - k % 2).wait_recv()
            along(q, k, 2).wait_recv()

    def near(k):
        return rem(y + 1 + 2 * rem(k, 2), NY)

    def other(k):
        return rem(y + 3 - 2 * rem(k, 2), NY)

    def far(n, k):
        return send(p_ref.at[n, k, far_y], r_ref.at[n, k], fs.at[n, k], fr.at[n, k], at(g, z, near(k), t))

    def plain(n, k):
        return send(p_ref.at[n, k, other(k)], u_ref.at[n, k], us.at[n, k], ur.at[n, k], at(g, z, other(k), t))

    def summed(n, k):
        return send(a_ref.at[n, k], w_ref.at[n, k], ws.at[n, k], wr.at[n, k], at(g, z, near(k), t))

    def back(n, k):
        return send(o_ref.at[n, k], e_ref.at[n, k], bs.at[n, k], br.at[n, k], at(g, z, y, rem(t + k, NT)))

    def experts(k):
        b = rem(t + k, NT)
        rows = jnp.concatenate(
            [x_ref[zi // 2, b, yi, :, (zi % 2) * FEAT:(zi % 2 + 1) * FEAT] for zi in range(NZ) for yi in range(NY)],
            axis=1,
        )
        wide = rows.astype(F32)
        scale = lax.rsqrt(jnp.sum(wide * wide, axis=1, keepdims=True) / MODEL + norm_eps)
        rows = (wide * scale).astype(BF)
        dims = (((1,), (1,)), ((), ()))
        gate = lax.dot_general(rows, gate_ref[...], dims, preferred_element_type=F32)
        up = lax.dot_general(rows, up_ref[...], dims, preferred_element_type=F32)
        h_ref[k] = (gate / (1.0 + jnp.exp(-gate)) * up).astype(BF)

    def products(n, k):
        hidden = h_ref[k]
        for i, zi in enumerate(HALVES[n]):
            part = jnp.dot(hidden, down_ref[:, zi * NY * FEAT:(zi + 1) * NY * FEAT], preferred_element_type=F32).astype(BF)
            for yi in range(NY):
                p_ref[n, k, yi, :, i * FEAT:(i + 1) * FEAT] = part[:, yi * FEAT:(yi + 1) * FEAT]

    def kth(i):
        return 4 + (1 - 2 * rem(i, 2)) * lax.div(i + 1, 2)

    def sweep0(i, _):
        k = kth(i)
        experts(k)
        products(0, k)
        far(0, k).start()
        plain(0, k).start()
        return 0

    def relay(n, k):
        far(n, k).wait_recv()
        a_ref[n, k] = (r_ref[n, k].astype(F32) + p_ref[n, k, near(k)].astype(F32)).astype(BF)
        summed(n, k).start()

    def finish(n, k):
        plain(n, k).wait_recv()
        summed(n, k).wait_recv()
        total = (p_ref[n, k, y].astype(F32) + u_ref[n, k].astype(F32) + w_ref[n, k].astype(F32)).astype(BF)

        @pl.when(k > 0)
        def _():
            o_ref[n, k] = total
            back(n, k).start()

        @pl.when(k == 0)
        def _():
            e_ref[n, k] = total

    def sweep1(i, _):
        k = kth(i)
        relay(0, k)
        products(1, k)
        far(1, k).start()
        plain(1, k).start()
        return 0

    def sweep2(i, _):
        k = kth(i)
        relay(1, k)
        finish(0, k)
        return 0

    def sweep3(i, _):
        finish(1, kth(i))
        return 0

    lax.fori_loop(0, NT, sweep0, 0)
    lax.fori_loop(0, NT, sweep1, 0)
    lax.fori_loop(0, NT, sweep2, 0)

    def combine(n):
        total = jnp.zeros((TOK, 2 * FEAT), F32)
        for k in FARS:
            if k:
                back(n, k).wait_recv()
            for i in range(2):
                total = total + jnp.dot(comb_ref[k, i], e_ref[n, k], preferred_element_type=F32)
        for i, zi in enumerate(HALVES[n]):
            m_ref[zi] = total[:, i * FEAT:(i + 1) * FEAT].astype(BF)

    def part(zi, zo):
        return send(m_ref.at[zo], l_ref.at[zi], cs.at[zo], cr.at[zi], at(g, zo, y, t))

    def home(n):
        for zo in HALVES[n]:
            @pl.when(zo != z)
            def _():
                part(z, zo).start()

    combine(0)
    home(0)
    lax.fori_loop(0, NT, sweep3, 0)
    combine(1)
    home(1)

    l_ref[z] = m_ref[z]
    own = jnp.zeros((TOK, FEAT), F32)
    for zi in range(NZ):
        @pl.when(zi != z)
        def _():
            part(zi, z).wait_recv()
    for zi in range(NZ):
        own = own + l_ref[zi].astype(F32)
    out_ref[...] = own.astype(BF)

    for m in served:
        m.wait()
    for i in (1, 2, 3):
        tok_copy(i).wait_send()
    for k in range(NT):
        for h in range(2):
            if k:
                first(k, h).wait_send()
            else:
                @pl.when(NC * c + h != y)
                def _():
                    first(k, h).wait_send()
    for j in range(NZ):
        for q in range(2):
            if j or q:
                second(j, q).wait_send()
    for n in range(2):
        for k in range(NT):
            for way in range(3):
                along(n, k, way).wait_send()
            if k:
                across(n, k).wait_send()
                back(n, k).wait_send()
            far(n, k).wait_send()
            plain(n, k).wait_send()
            summed(n, k).wait_send()
    for zo in range(NZ):
        @pl.when(zo != z)
        def _():
            part(z, zo).wait_send()


def local(tokens, routes, route_weight, norm_gain, gate_master, up_master, down_master):
    vm = pl.BlockSpec(memory_space=pltpu.VMEM)
    any_ = pl.BlockSpec(memory_space=pl.ANY)
    dma = pltpu.SemaphoreType.DMA
    serving = jax.ShapeDtypeStruct((1, COLS, MODEL), BF)
    master = pltpu.VMEM((EXPERTS, ROWS, WIDTH), F32)
    half = pltpu.VMEM((2, NT, CAP, 2 * FEAT), BF)
    mixed, gate_t, up_t, down_t = pl.pallas_call(
        kernel,
        out_shape=(jax.ShapeDtypeStruct((TOK, FEAT), BF), serving, serving, serving),
        in_specs=[vm, vm, vm, vm, any_, any_, any_],
        out_specs=(vm, any_, any_, any_),
        scratch_shapes=[
            master, master, master,
            pltpu.VMEM((16, TOK), F32),
            pltpu.VMEM((16, TOK), F32),
            pltpu.VMEM((NT, CAP, TOK), BF),
            pltpu.VMEM((NT, 2, TOK, CAP), BF),
            pltpu.VMEM((NT, 2, PACK, LANES), BF),
            pltpu.VMEM((NX, NY, PACK, LANES), BF),
            pltpu.VMEM((2 * NZ, NY, PACK, LANES), BF),
            pltpu.VMEM((NZ, TOK, FEAT), BF),
            half,
            pltpu.VMEM((2, NT, NY, CAP, 2 * FEAT), BF),
            pltpu.VMEM((COLS, MODEL), BF),
            pltpu.VMEM((COLS, MODEL), BF),
            pltpu.VMEM((COLS, MODEL), BF),
            pltpu.VMEM((NT, CAP, COLS), BF),
            pltpu.VMEM((2, NT, NY, CAP, 2 * FEAT), BF),
            half, half, half, half, half, half,
            pltpu.VMEM((NZ, TOK, FEAT), BF),
            pltpu.VMEM((NZ, TOK, FEAT), BF),
            dma((3,)), dma((NZ,)), dma((NZ,)),
            dma((NT, 2)), dma((NX * NY,)),
            dma((NZ, 2)), dma((NZ, 2)),
            dma((2, NT)), dma((2, NT)),
            dma((2, NT, 3)), dma((2, NT, 3)),
            dma((2, NT)), dma((2, NT)), dma((2, NT)), dma((2, NT)),
            dma((2, NT)), dma((2, NT)), dma((2, NT)), dma((2, NT)),
            dma((NZ,)), dma((NZ,)), dma((3,)),
        ],
        compiler_params=pltpu.CompilerParams(collective_id=0, has_side_effects=True, vmem_limit_bytes=VMEM_LIMIT),
        name="handover_kernel",
    )(tokens, routes.T, route_weight.T, norm_gain[None, :], gate_master, up_master, down_master)
    return mixed, jnp.swapaxes(gate_t, 1, 2), jnp.swapaxes(up_t, 1, 2), jnp.swapaxes(down_t, 1, 2)


def solution(mesh):
    placed = (
        P(("gr", "tp"), "fs"),
        P(("gr", "tp"), None),
        P(("gr", "tp"), None),
        P(("gr", "fs")),
        P(None, ("gr", "fs"), "tp"),
        P(None, ("gr", "fs"), "tp"),
        P(None, ("gr", "fs"), "tp"),
    )
    return jax.shard_map(
        local,
        mesh=mesh,
        in_specs=placed,
        out_specs=(
            P(("gr", "tp"), "fs"),
            P("tp", None, "fs"),
            P("tp", None, "fs"),
            P("tp", None, "fs"),
        ),
        check_vma=False,
    )
```

```python
import jax
import jax.numpy as jnp
from jax import lax
from jax.experimental import pallas as pl
from jax.experimental.pallas import tpu as pltpu
from jax.sharding import PartitionSpec as P

norm_eps = 1e-06
BF = jnp.bfloat16
F32 = jnp.float32
I32 = jnp.int32
MESH = pl.DeviceIdType.MESH
VMEM_LIMIT = 60 * 1024 * 1024

NY, NZ, NX, NC = 4, 4, 4, 2
NT = NX * NC
EXPERTS = 8
CAP = 192
ROWS = 64
WIDTH = 352
COLS = 176
LANES = 128
DLO, DHI = 96, 80
PACK = COLS + DLO
TOK = 512
FEAT = 128
MODEL = 2048
NEAR = (0, 1, 7, 2, 6, 3, 5, 4)
FARS = (4, 3, 5, 2, 6, 1, 7, 0)
PARTS = ((0, 3), (2,))
LATE = 1


def rem(a, n):
    return lax.rem(a, n)


def at(g, z, y, t):
    return (g, z * NY + y, t)


def send(src, dst, ss, rs, to):
    return pltpu.make_async_remote_copy(
        src_ref=src, dst_ref=dst, send_sem=ss, recv_sem=rs, device_id=to, device_id_type=MESH
    )


def kernel(
    tok_ref, routes_ref, weight_ref, gain_ref, gm_hbm, um_hbm, dm_hbm,
    out_ref, gate_out, up_out, down_out,
    gm_ref, um_ref, dm_ref, key_ref, mix_ref, table_ref, comb_ref,
    wp_ref, q_ref, v_ref, t_ref, ty_ref, s0_ref, s1_ref, s2_ref, x_ref, gate_ref, up_ref, down_ref, h_ref,
    p0, r0, a0, u0, w0, o0, e0, p1, r1, a1, u1, w1, o1, e1, pl_ref, el_ref, my_ref, ly_ref, m_ref, l_ref,
    ms, zs, zr, tys, tyr, qs, qr, vs, vr, xs, xr, ys, yr,
    fs, fr, us, ur, ws, wr, bs, br, ds, dr, cs, cr, outs,
):
    ps, rs_, as_, us_, ws_, os_, es = ((p0, p1), (r0, r1), (a0, a1), (u0, u1), (w0, w1), (o0, o1), (e0, e1))
    g, f, t = lax.axis_index("gr"), lax.axis_index("fs"), lax.axis_index("tp")
    z, y = lax.div(f, NY), rem(f, NY)
    x, c = lax.div(t, NC), rem(t, NC)
    up_y, dn_y, far_y = rem(y + 1, NY), rem(y + NY - 1, NY), rem(y + 2, NY)

    masters = [
        pltpu.make_async_copy(src, dst, ms.at[i])
        for i, (src, dst) in enumerate(((gm_hbm, gm_ref), (um_hbm, um_ref), (dm_hbm, dm_ref)))
    ]
    for m in masters:
        m.start()

    barrier = pltpu.get_barrier_semaphore()
    count = 0
    for dy in range(NY):
        for dt in range(NT):
            if dy or dt:
                pl.semaphore_signal(barrier, inc=1, device_id=at(g, z, rem(y + dy, NY), rem(t + dt, NT)), device_id_type=MESH)
                count += 1
    for dg in range(2):
        for dz in range(NZ):
            if dg or dz:
                pl.semaphore_signal(barrier, inc=1, device_id=at(rem(g + dg, 2), rem(z + dz, NZ), y, t), device_id_type=MESH)
                count += 1

    ex = lax.broadcasted_iota(I32, (16, TOK), 0)
    first_is, second_is = routes_ref[0:1, :] == ex, routes_ref[1:2, :] == ex
    named = first_is | second_is
    before = lax.broadcasted_iota(I32, (TOK, TOK), 0) < lax.broadcasted_iota(I32, (TOK, TOK), 1)
    rank = jnp.dot(
        jnp.where(named, 1.0, 0.0).astype(BF), jnp.where(before, 1.0, 0.0).astype(BF), preferred_element_type=F32
    )
    key_ref[...] = jnp.where(named, rank, -1.0)
    mix_ref[...] = jnp.where(first_is, weight_ref[0:1, :], 0.0) + jnp.where(second_is, weight_ref[1:2, :], 0.0)
    slot = lax.broadcasted_iota(I32, (CAP, TOK), 0).astype(F32)

    def tables(k, _):
        key = key_ref[pl.ds(rem(t + k, NT), 1), :]
        table_ref[k] = jnp.where(slot == key, 1.0, 0.0).astype(BF)
        return 0

    lax.fori_loop(0, NT, tables, 0)
    ty_ref[y] = tok_ref[...]

    pl.semaphore_wait(barrier, count)

    low, base = rem(z, 2), 2 * lax.div(z, 2)
    peers = {1: base + 1 - low, 2: 2 - base + low, 3: 3 - base - low}

    def tok_copy(i):
        return send(tok_ref, t_ref.at[z], zs.at[i], zr.at[i], at(g, peers[i], y, t))

    def tok_along(i):
        return send(tok_ref, ty_ref.at[y], tys.at[i], tyr.at[i], at(g, z, rem(y + i, NY), t))

    for i in (1, 2, 3):
        tok_copy(i).start()
    for i in (1, 3, 2):
        tok_along(i).start()

    def first(k, h):
        return send(
            wp_ref.at[k, h], q_ref.at[x, y], qs.at[k, h], qr.at[x * NY + y],
            at(g, z, NC * c + h, rem(t + k, NT)),
        )

    def first_start(k):
        for h in range(2):
            mine = (NC * c + h == y) & (rem(t + k, NT) == t)

            @pl.when(mine)
            def _():
                pltpu.make_async_copy(wp_ref.at[k, h], q_ref.at[x, y], qr.at[x * NY + y]).start()

            @pl.when(jnp.logical_not(mine))
            def _():
                first(k, h).start()

    for m in masters:
        m.wait()
    gain = jnp.concatenate([gain_ref[...], gain_ref[...]], axis=1)

    def pack(i, _):
        k = 4 + (1 - 2 * rem(i, 2)) * lax.div(i + 1, 2)
        e = rem(t + k, NT)
        pad = jnp.zeros((2 * ROWS, 3 * LANES - WIDTH), F32)
        gu = jnp.concatenate([gm_ref[e], um_ref[e]], axis=0)
        gu = (jnp.transpose(jnp.concatenate([gu, pad], axis=1)) * gain).astype(BF)
        dn = dm_ref[e]
        dn = jnp.concatenate([dn, pad[:ROWS]], axis=1)
        dd = jnp.concatenate([dn, pltpu.roll(dn, 3 * LANES - DLO, 1)], axis=0)
        dd = jnp.transpose(dd).astype(BF)
        for h in range(2):
            lo = h * COLS
            wp_ref[k, h, 0:COLS, :] = gu[lo:lo + COLS]
            wp_ref[k, h, COLS:PACK, :] = dd[lo:lo + DLO]

        @pl.when(i > 0)
        def _():
            j = i - 1
            first_start(4 + (1 - 2 * rem(j, 2)) * lax.div(j + 1, 2))

        return 0

    lax.fori_loop(0, NT, pack, 0)
    first_start(0)

    mate, rest = peers[1], 2 - base
    tiles = (mate, pl.ds(rest, 2))
    stage = (s0_ref, s1_ref)

    def dispatch(q):
        rows_in = t_ref[mate] if q == 0 else jnp.concatenate([t_ref[rest], t_ref[rest + 1]], axis=1)
        for k in NEAR:
            rows = jnp.dot(table_ref[k], rows_in, preferred_element_type=F32).astype(BF)
            for i in range(1 + q):
                part = rows[:, i * FEAT:(i + 1) * FEAT]
                if k == 0:
                    x_ref[rest + i if q else mate, t, y] = part
                elif q:
                    s1_ref[k, i] = part
                else:
                    s0_ref[k] = part

    def dispatch_own():
        rows_in = jnp.concatenate([ty_ref[i] for i in range(NY)], axis=1)
        for k in NEAR:
            rows = jnp.dot(table_ref[k], rows_in, preferred_element_type=F32).astype(BF)
            for i in range(NY):
                part = rows[:, i * FEAT:(i + 1) * FEAT]
                if k == 0:
                    x_ref[z, t, i] = part
                else:
                    s2_ref[k, i] = part

    def across(q, k):
        if q == 2:
            src, dst = s2_ref.at[k], x_ref.at[z, t]
        else:
            src, dst = stage[q].at[k], x_ref.at[tiles[q], t, y]
        return send(src, dst, xs.at[q, k], xr.at[q, k], at(g, z, y, rem(t + k, NT)))

    def along(q, k, way):
        b = rem(t + NT - k, NT)
        whose = y if way < 2 else (dn_y if k % 2 == 0 else up_y)
        to = up_y if way == 0 or (way == 2 and k % 2 == 0) else dn_y
        ref = x_ref.at[tiles[q], b, whose]
        return send(ref, ref, ys.at[q, k, way], yr.at[q, k, way], at(g, z, to, t))

    def spread(q, k):
        if k:
            across(q, k).wait_recv()
        along(q, k, 0).start()
        along(q, k, 1).start()

    def forward(q, k):
        along(q, k, k % 2).wait_recv()
        along(q, k, 2).start()

    zz = g * NZ + z

    def second(j, q):
        zd = rem(z + j, NZ)
        return send(q_ref.at[zd], v_ref.at[zz], vs.at[j, q], vr.at[j, q], at(rem(g + q, 2), zd, y, t))

    own_v = pltpu.make_async_copy(q_ref.at[z], v_ref.at[zz], vr.at[0, 0])

    def weights_on(j):
        zd = rem(z + j, NZ)
        for i in range(NY):
            send(q_ref.at[zd, i], q_ref.at[zd, i], qs.at[0, 0], qr.at[zd * NY + i], at(g, z, up_y, t)).wait_recv()
        for q in (1, 0):
            if j or q:
                second(j, q).start()
            else:
                own_v.start()

    tok_copy(1).wait_recv()
    dispatch(0)
    for k in NEAR[1:]:
        across(0, k).start()
    spread(0, 0)
    tok_copy(2).wait_recv()
    tok_copy(3).wait_recv()
    dispatch(1)
    for k in NEAR[1:]:
        across(1, k).start()
    spread(1, 0)
    for i in (1, 3, 2):
        tok_along(i).wait_recv()
    dispatch_own()
    for k in FARS[:-1]:
        across(2, k).start()
    for j in (2, 1, 3, 0):
        weights_on(j)
    for k in NEAR[1:]:
        spread(0, k)
    for k in NEAR:
        forward(0, k)
        if k:
            spread(1, k)
    for k in NEAR:
        forward(1, k)

    def weighting(k, _):
        e = rem(t + NT - k, NT)
        here = slot == key_ref[pl.ds(e, 1), :]
        mix = mix_ref[pl.ds(e, 1), :]
        high = mix.astype(BF).astype(F32)
        for i, part in enumerate((high, mix - high)):
            comb_ref[k, i] = jnp.transpose(jnp.where(here, part, 0.0)).astype(BF)
        return 0

    lax.fori_loop(0, NT, weighting, 0)

    left = lax.broadcasted_iota(I32, (COLS, LANES), 1) < ROWS

    def unpack(zs_):
        for i in range(NY // 2):
            a, b = (v_ref[zs_, 2 * i + n].astype(F32) for n in range(2))
            ra, rb = pltpu.roll(a, ROWS, 1), pltpu.roll(b, ROWS, 1)
            cols = pl.ds(pl.multiple_of((zs_ * (NY // 2) + i) * LANES, LANES), LANES)
            gate_ref[:, cols] = jnp.where(left, a[:COLS], rb[:COLS]).astype(BF)
            up_ref[:, cols] = jnp.where(left, ra[:COLS], b[:COLS]).astype(BF)
            down_ref[0:DLO, cols] = jnp.where(left[:DLO], a[COLS:], rb[COLS:]).astype(BF)
            down_ref[DLO:COLS, cols] = jnp.where(left[:DHI], ra[COLS:COLS + DHI], b[COLS:COLS + DHI]).astype(BF)

    own_v.wait()
    unpack(zz)
    for j, q in ((1, 0), (3, 0), (2, 0), (1, 1), (3, 1), (2, 1), (0, 1)):
        second(j, q).wait_recv()
        unpack(rem(g + q, 2) * NZ + rem(z + NZ - j, NZ))
    served = [
        pltpu.make_async_copy(src, dst.at[0], outs.at[i])
        for i, (src, dst) in enumerate(((gate_ref, gate_out), (up_ref, up_out), (down_ref, down_out)))
    ]
    for m in served:
        m.start()

    for q in range(2):
        for k in NEAR:
            along(q, k, 1 - k % 2).wait_recv()
            along(q, k, 2).wait_recv()
    for k in FARS[:-1]:
        across(2, k).wait_recv()

    def near(k):
        return rem(y + 1 + 2 * rem(k, 2), NY)

    def other(k):
        return rem(y + 3 - 2 * rem(k, 2), NY)

    def far(n, k):
        return send(ps[n].at[k, far_y], rs_[n].at[k], fs.at[n, k], fr.at[n, k], at(g, z, near(k), t))

    def plain(n, k):
        return send(ps[n].at[k, other(k)], us_[n].at[k], us.at[n, k], ur.at[n, k], at(g, z, other(k), t))

    def summed(n, k):
        return send(as_[n].at[k], ws_[n].at[k], ws.at[n, k], wr.at[n, k], at(g, z, near(k), t))

    def back(n, k):
        src, dst = (os_[n].at[k], es[n].at[k]) if n < 2 else (pl_ref.at[k], el_ref.at[k])
        return send(src, dst, bs.at[n, k], br.at[n, k], at(g, z, y, rem(t + k, NT)))

    def experts(k):
        b = rem(t + k, NT)
        rows = jnp.concatenate(
            [x_ref[zi, b, yi] for zi in range(NZ) for yi in range(NY)],
            axis=1,
        )
        wide = rows.astype(F32)
        scale = lax.rsqrt(jnp.sum(wide * wide, axis=1, keepdims=True) / MODEL + norm_eps)
        rows = (wide * scale).astype(BF)
        dims = (((1,), (1,)), ((), ()))
        gate = lax.dot_general(rows, gate_ref[...], dims, preferred_element_type=F32)
        up = lax.dot_general(rows, up_ref[...], dims, preferred_element_type=F32)
        h_ref[k] = (gate / (1.0 + jnp.exp(-gate)) * up).astype(BF)

    def product(zi, k):
        cols = slice(zi * NY * FEAT, (zi + 1) * NY * FEAT)
        return jnp.dot(h_ref[k], down_ref[:, cols], preferred_element_type=F32).astype(BF)

    def products(n, k):
        for i, zi in enumerate(PARTS[n]):
            part = product(zi, k)
            for yi in range(NY):
                ps[n][k, yi, :, i * FEAT:(i + 1) * FEAT] = part[:, yi * FEAT:(yi + 1) * FEAT]

    def kth(i):
        return 4 + (1 - 2 * rem(i, 2)) * lax.div(i + 1, 2)

    def sweep0(i, _):
        k = kth(i)
        experts(k)
        products(0, k)
        late = product(LATE, k)
        far(0, k).start()
        plain(0, k).start()

        @pl.when(k > 0)
        def _():
            pl_ref[k] = late
            back(2, k).start()

        @pl.when(k == 0)
        def _():
            el_ref[k] = late

        return 0

    def relay(n, k):
        far(n, k).wait_recv()
        as_[n][k] = (rs_[n][k].astype(F32) + ps[n][k, near(k)].astype(F32)).astype(BF)
        summed(n, k).start()

    def finish(n, k):
        plain(n, k).wait_recv()
        summed(n, k).wait_recv()
        total = (ps[n][k, y].astype(F32) + us_[n][k].astype(F32) + ws_[n][k].astype(F32)).astype(BF)

        @pl.when(k > 0)
        def _():
            os_[n][k] = total
            back(n, k).start()

        @pl.when(k == 0)
        def _():
            es[n][k] = total

    def sweep1(i, _):
        k = kth(i)
        relay(0, k)
        products(1, k)
        far(1, k).start()
        plain(1, k).start()
        return 0

    def sweep2(i, _):
        k = kth(i)
        relay(1, k)
        finish(0, k)
        return 0

    def sweep3(i, _):
        finish(1, kth(i))
        return 0

    def combined(n):
        rows = es[n] if n < 2 else el_ref
        total = jnp.zeros((TOK, rows.shape[-1]), F32)
        for k in FARS:
            if k:
                back(n, k).wait_recv()
            for i in range(2):
                total = total + jnp.dot(comb_ref[k, i], rows[k], preferred_element_type=F32)
        return total

    def token_sum(i):
        to = rem(y + i, NY)
        return send(my_ref.at[to], ly_ref.at[y], ds.at[i], dr.at[i], at(g, z, to, t))

    def part(zi, zo):
        return send(m_ref.at[zo], l_ref.at[zi], cs.at[zo], cr.at[zi], at(g, zo, y, t))

    def home(zo):
        @pl.when(zo != z)
        def _():
            part(z, zo).start()

    def combine(n):
        total = combined(n)
        for i, zo in enumerate(PARTS[n]):
            m_ref[zo] = total[:, i * FEAT:(i + 1) * FEAT].astype(BF)
        for zo in PARTS[n]:
            home(zo)

    lax.fori_loop(0, NT, sweep0, 0)
    lax.fori_loop(0, NT, sweep1, 0)
    total = combined(2)
    for i in range(NY):
        my_ref[i] = total[:, i * FEAT:(i + 1) * FEAT].astype(BF)
    for i in (1, 3, 2):
        token_sum(i).start()
    lax.fori_loop(0, NT, sweep2, 0)
    combine(0)
    ly_ref[y] = my_ref[y]
    for i in (1, 3, 2):
        token_sum(i).wait_recv()
    total = jnp.zeros((TOK, FEAT), F32)
    for i in range(NY):
        total = total + ly_ref[i].astype(F32)
    m_ref[LATE] = total.astype(BF)
    home(LATE)
    lax.fori_loop(0, NT, sweep3, 0)
    combine(1)

    l_ref[z] = m_ref[z]
    own = jnp.zeros((TOK, FEAT), F32)
    for zi in range(NZ):
        @pl.when(zi != z)
        def _():
            part(zi, z).wait_recv()
    for zi in range(NZ):
        own = own + l_ref[zi].astype(F32)
    out_ref[...] = own.astype(BF)

    for m in served:
        m.wait()
    for i in (1, 2, 3):
        tok_copy(i).wait_send()
        tok_along(i).wait_send()
        token_sum(i).wait_send()
    for k in range(NT):
        for h in range(2):
            if k:
                first(k, h).wait_send()
            else:
                @pl.when(NC * c + h != y)
                def _():
                    first(k, h).wait_send()
    for j in range(NZ):
        for q in range(2):
            if j or q:
                second(j, q).wait_send()
    for k in range(1, NT):
        across(2, k).wait_send()
        back(2, k).wait_send()
    for n in range(2):
        for k in range(NT):
            for way in range(3):
                along(n, k, way).wait_send()
            if k:
                across(n, k).wait_send()
                back(n, k).wait_send()
            far(n, k).wait_send()
            plain(n, k).wait_send()
            summed(n, k).wait_send()
    for zo in range(NZ):
        @pl.when(zo != z)
        def _():
            part(z, zo).wait_send()


def hand_over(*refs):
    src, dst, held, ins, outs = refs[:4], refs[4:8], refs[8:12], refs[12], refs[13]
    reads = [pltpu.make_async_copy(src[i], held[i], ins.at[i]) for i in range(4)]
    writes = [pltpu.make_async_copy(held[i], dst[i], outs.at[i]) for i in range(4)]
    for r in reads:
        r.start()
    for r, w in zip(reads, writes):
        r.wait()
        w.start()
    for w in writes:
        w.wait()


def local(tokens, routes, route_weight, norm_gain, gate_master, up_master, down_master):
    vm = pl.BlockSpec(memory_space=pltpu.VMEM)
    any_ = pl.BlockSpec(memory_space=pl.ANY)
    dma = pltpu.SemaphoreType.DMA
    serving = jax.ShapeDtypeStruct((1, COLS, MODEL), BF)
    mixed = jax.ShapeDtypeStruct((TOK, FEAT), BF)
    master = pltpu.VMEM((EXPERTS, ROWS, WIDTH), F32)

    def rows(*dims):
        return pltpu.VMEM((*dims[:-1], CAP, dims[-1]), BF)

    def summing(width):
        return [rows(NT, NY, width)] + [rows(NT, width)] * 6

    shapes = (mixed, serving, serving, serving)
    results = pl.pallas_call(
        kernel,
        out_shape=shapes,
        in_specs=[vm, vm, vm, vm, any_, any_, any_],
        out_specs=(vm, any_, any_, any_),
        scratch_shapes=[
            master, master, master,
            pltpu.VMEM((16, TOK), F32),
            pltpu.VMEM((16, TOK), F32),
            pltpu.VMEM((NT, CAP, TOK), BF),
            pltpu.VMEM((NT, 2, TOK, CAP), BF),
            pltpu.VMEM((NT, 2, PACK, LANES), BF),
            pltpu.VMEM((NX, NY, PACK, LANES), BF),
            pltpu.VMEM((2 * NZ, NY, PACK, LANES), BF),
            pltpu.VMEM((NZ, TOK, FEAT), BF),
            pltpu.VMEM((NY, TOK, FEAT), BF),
            rows(NT, FEAT), rows(NT, 2, FEAT), rows(NT, NY, FEAT),
            rows(NZ, NT, NY, FEAT),
            pltpu.VMEM((COLS, MODEL), BF),
            pltpu.VMEM((COLS, MODEL), BF),
            pltpu.VMEM((COLS, MODEL), BF),
            rows(NT, COLS),
            *summing(2 * FEAT), *summing(FEAT),
            rows(NT, NY * FEAT), rows(NT, NY * FEAT),
            pltpu.VMEM((NY, TOK, FEAT), BF),
            pltpu.VMEM((NY, TOK, FEAT), BF),
            pltpu.VMEM((NZ, TOK, FEAT), BF),
            pltpu.VMEM((NZ, TOK, FEAT), BF),
            dma((3,)), dma((NZ,)), dma((NZ,)), dma((NY,)), dma((NY,)),
            dma((NT, 2)), dma((NX * NY,)),
            dma((NZ, 2)), dma((NZ, 2)),
            dma((3, NT)), dma((3, NT)),
            dma((2, NT, 3)), dma((2, NT, 3)),
            dma((2, NT)), dma((2, NT)), dma((2, NT)), dma((2, NT)),
            dma((2, NT)), dma((2, NT)), dma((3, NT)), dma((3, NT)),
            dma((NY,)), dma((NY,)),
            dma((NZ,)), dma((NZ,)), dma((3,)),
        ],
        compiler_params=pltpu.CompilerParams(collective_id=0, has_side_effects=True, vmem_limit_bytes=VMEM_LIMIT),
        name="handover_kernel",
    )(tokens, routes.T, route_weight.T, norm_gain[None, :], gate_master, up_master, down_master)
    out, gate_t, up_t, down_t = pl.pallas_call(
        hand_over,
        out_shape=shapes,
        in_specs=[any_] * 4,
        out_specs=(any_,) * 4,
        scratch_shapes=[pltpu.VMEM(v.shape, BF) for v in shapes] + [dma((4,)), dma((4,))],
        name="output_kernel",
    )(*results)
    return out, jnp.swapaxes(gate_t, 1, 2), jnp.swapaxes(up_t, 1, 2), jnp.swapaxes(down_t, 1, 2)


def solution(mesh):
    placed = (
        P(("gr", "tp"), "fs"),
        P(("gr", "tp"), None),
        P(("gr", "tp"), None),
        P(("gr", "fs")),
        P(None, ("gr", "fs"), "tp"),
        P(None, ("gr", "fs"), "tp"),
        P(None, ("gr", "fs"), "tp"),
    )
    return jax.shard_map(
        local,
        mesh=mesh,
        in_specs=placed,
        out_specs=(
            P(("gr", "tp"), "fs"),
            P("tp", None, "fs"),
            P("tp", None, "fs"),
            P("tp", None, "fs"),
        ),
        check_vma=False,
    )
```

```python
import jax
import jax.numpy as jnp
from jax import lax
from jax.experimental import pallas as pl
from jax.experimental.pallas import tpu as pltpu
from jax.sharding import PartitionSpec as P

norm_eps = 1e-06
BF = jnp.bfloat16
F32 = jnp.float32
I32 = jnp.int32
MESH = pl.DeviceIdType.MESH
VMEM_LIMIT = 60 * 1024 * 1024

NY, NZ, NX, NC = 4, 4, 4, 2
NT = NX * NC
EXPERTS = 8
CAP = 192
ROWS = 64
WIDTH = 352
COLS = 176
LANES = 128
DLO, DHI = 96, 80
PACK = COLS + DLO
TOK = 512
FEAT = 128
MODEL = 2048
NEAR = (0, 1, 7, 2, 6, 3, 5, 4)
FARS = (4, 3, 5, 2, 6, 1, 7, 0)
PARTS = ((0, 3), (2,))
LATE = 1


def rem(a, n):
    return lax.rem(a, n)


def at(g, z, y, t):
    return (g, z * NY + y, t)


def send(src, dst, ss, rs, to):
    return pltpu.make_async_remote_copy(
        src_ref=src, dst_ref=dst, send_sem=ss, recv_sem=rs, device_id=to, device_id_type=MESH
    )


def kernel(
    tok_ref, routes_ref, weight_ref, gain_ref, gm_hbm, um_hbm, dm_hbm,
    out_ref, gate_out, up_out, down_out,
    gm_ref, um_ref, dm_ref, key_ref, mix_ref, table_ref, comb_ref,
    wp_ref, q_ref, v_ref, t_ref, ty_ref, s0_ref, s1_ref, s2_ref, x_ref, gate_ref, up_ref, down_ref, h_ref,
    p0, r0, a0, u0, w0, o0, e0, p1, r1, a1, u1, w1, o1, e1, pl_ref, el_ref, my_ref, ly_ref, m_ref, l_ref,
    ms, zs, zr, tys, tyr, qs, qr, vs, vr, xs, xr, ys, yr,
    fs, fr, us, ur, ws, wr, bs, br, ds, dr, cs, cr, outs,
):
    ps, rs_, as_, us_, ws_, os_, es = ((p0, p1), (r0, r1), (a0, a1), (u0, u1), (w0, w1), (o0, o1), (e0, e1))
    g, f, t = lax.axis_index("gr"), lax.axis_index("fs"), lax.axis_index("tp")
    z, y = lax.div(f, NY), rem(f, NY)
    x, c = lax.div(t, NC), rem(t, NC)
    up_y, dn_y, far_y = rem(y + 1, NY), rem(y + NY - 1, NY), rem(y + 2, NY)

    masters = [
        pltpu.make_async_copy(src, dst, ms.at[i])
        for i, (src, dst) in enumerate(((gm_hbm, gm_ref), (um_hbm, um_ref), (dm_hbm, dm_ref)))
    ]
    for m in masters:
        m.start()

    barrier = pltpu.get_barrier_semaphore()
    count = 0
    for dy in range(NY):
        for dt in range(NT):
            if dy or dt:
                pl.semaphore_signal(barrier, inc=1, device_id=at(g, z, rem(y + dy, NY), rem(t + dt, NT)), device_id_type=MESH)
                count += 1
    for dg in range(2):
        for dz in range(NZ):
            if dg or dz:
                pl.semaphore_signal(barrier, inc=1, device_id=at(rem(g + dg, 2), rem(z + dz, NZ), y, t), device_id_type=MESH)
                count += 1

    ex = lax.broadcasted_iota(I32, (16, TOK), 0)
    first_is, second_is = routes_ref[0:1, :] == ex, routes_ref[1:2, :] == ex
    named = first_is | second_is
    before = lax.broadcasted_iota(I32, (TOK, TOK), 0) < lax.broadcasted_iota(I32, (TOK, TOK), 1)
    rank = jnp.dot(
        jnp.where(named, 1.0, 0.0).astype(BF), jnp.where(before, 1.0, 0.0).astype(BF), preferred_element_type=F32
    )
    key_ref[...] = jnp.where(named, rank, -1.0)
    mix_ref[...] = jnp.where(first_is, weight_ref[0:1, :], 0.0) + jnp.where(second_is, weight_ref[1:2, :], 0.0)
    slot = lax.broadcasted_iota(I32, (CAP, TOK), 0).astype(F32)

    def tables(k, _):
        key = key_ref[pl.ds(rem(t + k, NT), 1), :]
        table_ref[k] = jnp.where(slot == key, 1.0, 0.0).astype(BF)
        return 0

    lax.fori_loop(0, NT, tables, 0)
    ty_ref[y] = tok_ref[...]

    def weighting(k, _):
        e = rem(t + NT - k, NT)
        here = slot == key_ref[pl.ds(e, 1), :]
        mix = mix_ref[pl.ds(e, 1), :]
        high = mix.astype(BF).astype(F32)
        for i, part in enumerate((high, mix - high)):
            comb_ref[k, i] = jnp.transpose(jnp.where(here, part, 0.0)).astype(BF)
        return 0

    lax.fori_loop(0, NT, weighting, 0)

    for m in masters:
        m.wait()
    gain = jnp.concatenate([gain_ref[...], gain_ref[...]], axis=1)

    def pack(i, _):
        k = 4 + (1 - 2 * rem(i, 2)) * lax.div(i + 1, 2)
        e = rem(t + k, NT)
        pad = jnp.zeros((2 * ROWS, 3 * LANES - WIDTH), F32)
        gu = jnp.concatenate([gm_ref[e], um_ref[e]], axis=0)
        gu = (jnp.transpose(jnp.concatenate([gu, pad], axis=1)) * gain).astype(BF)
        dn = dm_ref[e]
        dn = jnp.concatenate([dn, pad[:ROWS]], axis=1)
        dd = jnp.concatenate([dn, pltpu.roll(dn, 3 * LANES - DLO, 1)], axis=0)
        dd = jnp.transpose(dd).astype(BF)
        for h in range(2):
            lo = h * COLS
            wp_ref[k, h, 0:COLS, :] = gu[lo:lo + COLS]
            wp_ref[k, h, COLS:PACK, :] = dd[lo:lo + DLO]

        return 0

    lax.fori_loop(0, NT, pack, 0)
    pl.semaphore_wait(barrier, count)

    low, base = rem(z, 2), 2 * lax.div(z, 2)
    peers = {1: base + 1 - low, 2: 2 - base + low, 3: 3 - base - low}

    def tok_copy(i):
        return send(tok_ref, t_ref.at[z], zs.at[i], zr.at[i], at(g, peers[i], y, t))

    def tok_along(i):
        return send(tok_ref, ty_ref.at[y], tys.at[i], tyr.at[i], at(g, z, rem(y + i, NY), t))

    for i in (1, 2, 3):
        tok_copy(i).start()
    def first(k, h):
        return send(
            wp_ref.at[k, h], q_ref.at[x, y], qs.at[k, h], qr.at[x * NY + y],
            at(g, z, NC * c + h, rem(t + k, NT)),
        )

    def first_start(k):
        for h in range(2):
            mine = (NC * c + h == y) & (rem(t + k, NT) == t)

            @pl.when(mine)
            def _():
                pltpu.make_async_copy(wp_ref.at[k, h], q_ref.at[x, y], qr.at[x * NY + y]).start()

            @pl.when(jnp.logical_not(mine))
            def _():
                first(k, h).start()

    for k in FARS:
        first_start(k)
    for i in (1, 3, 2):
        tok_along(i).start()

    mate, rest = peers[1], 2 - base
    tiles = (mate, pl.ds(rest, 2))
    stage = (s0_ref, s1_ref)

    def dispatch(q):
        rows_in = t_ref[mate] if q == 0 else jnp.concatenate([t_ref[rest], t_ref[rest + 1]], axis=1)
        for k in NEAR:
            rows = jnp.dot(table_ref[k], rows_in, preferred_element_type=F32).astype(BF)
            for i in range(1 + q):
                part = rows[:, i * FEAT:(i + 1) * FEAT]
                if k == 0:
                    x_ref[rest + i if q else mate, t, y] = part
                elif q:
                    s1_ref[k, i] = part
                else:
                    s0_ref[k] = part

    def dispatch_own():
        rows_in = jnp.concatenate([ty_ref[i] for i in range(NY)], axis=1)
        for k in NEAR:
            rows = jnp.dot(table_ref[k], rows_in, preferred_element_type=F32).astype(BF)
            for i in range(NY):
                part = rows[:, i * FEAT:(i + 1) * FEAT]
                if k == 0:
                    x_ref[z, t, i] = part
                else:
                    s2_ref[k, i] = part

    def across(q, k):
        if q == 2:
            src, dst = s2_ref.at[k], x_ref.at[z, t]
        else:
            src, dst = stage[q].at[k], x_ref.at[tiles[q], t, y]
        return send(src, dst, xs.at[q, k], xr.at[q, k], at(g, z, y, rem(t + k, NT)))

    def along(q, k, way):
        b = rem(t + NT - k, NT)
        whose = y if way < 2 else (dn_y if k % 2 == 0 else up_y)
        to = up_y if way == 0 or (way == 2 and k % 2 == 0) else dn_y
        ref = x_ref.at[tiles[q], b, whose]
        return send(ref, ref, ys.at[q, k, way], yr.at[q, k, way], at(g, z, to, t))

    def spread(q, k):
        if k:
            across(q, k).wait_recv()
        along(q, k, 0).start()
        along(q, k, 1).start()

    def forward(q, k):
        along(q, k, k % 2).wait_recv()
        along(q, k, 2).start()

    zz = g * NZ + z

    def second(j, q):
        zd = rem(z + j, NZ)
        return send(q_ref.at[zd], v_ref.at[zz], vs.at[j, q], vr.at[j, q], at(rem(g + q, 2), zd, y, t))

    own_v = pltpu.make_async_copy(q_ref.at[z], v_ref.at[zz], vr.at[0, 0])
    feeder = lax.div(y, NC)
    odd = rem(c + feeder, NC)

    def weights_on(i):
        k = (4, 2, 6, 0)[i] + odd * (-1, 3, -5, 7)[i]
        zd = lax.div(rem(t + NT - k, NT), NC)
        for n in range(NY):
            send(q_ref.at[zd, n], q_ref.at[zd, n], qs.at[0, 0], qr.at[zd * NY + n], at(g, z, up_y, t)).wait_recv()
        j = rem(zd + NZ - z, NZ)
        second(j, 1).start()

        @pl.when(j > 0)
        def _():
            second(j, 0).start()

        @pl.when(j == 0)
        def _():
            own_v.start()

    tok_copy(1).wait_recv()
    dispatch(0)
    for k in NEAR[1:]:
        across(0, k).start()
    spread(0, 0)
    weights_on(0)
    weights_on(1)
    tok_copy(2).wait_recv()
    tok_copy(3).wait_recv()
    dispatch(1)
    for k in NEAR[1:]:
        across(1, k).start()
    spread(1, 0)
    weights_on(2)
    weights_on(3)
    for i in (1, 3, 2):
        tok_along(i).wait_recv()
    dispatch_own()
    for k in FARS[:-1]:
        across(2, k).start()
    for k in NEAR[1:]:
        spread(0, k)
    for k in NEAR:
        forward(0, k)
        if k:
            spread(1, k)
    for k in NEAR:
        forward(1, k)

    left = lax.broadcasted_iota(I32, (COLS, LANES), 1) < ROWS

    def unpack(zs_):
        for i in range(NY // 2):
            a, b = (v_ref[zs_, 2 * i + n].astype(F32) for n in range(2))
            ra, rb = pltpu.roll(a, ROWS, 1), pltpu.roll(b, ROWS, 1)
            cols = pl.ds(pl.multiple_of((zs_ * (NY // 2) + i) * LANES, LANES), LANES)
            gate_ref[:, cols] = jnp.where(left, a[:COLS], rb[:COLS]).astype(BF)
            up_ref[:, cols] = jnp.where(left, ra[:COLS], b[:COLS]).astype(BF)
            down_ref[0:DLO, cols] = jnp.where(left[:DLO], a[COLS:], rb[COLS:]).astype(BF)
            down_ref[DLO:COLS, cols] = jnp.where(left[:DHI], ra[COLS:COLS + DHI], b[COLS:COLS + DHI]).astype(BF)

    own_v.wait()
    unpack(zz)
    for j, q in ((1, 0), (3, 0), (2, 0), (1, 1), (3, 1), (2, 1), (0, 1)):
        second(j, q).wait_recv()
        unpack(rem(g + q, 2) * NZ + rem(z + NZ - j, NZ))
    served = [
        pltpu.make_async_copy(src, dst.at[0], outs.at[i])
        for i, (src, dst) in enumerate(((gate_ref, gate_out), (up_ref, up_out), (down_ref, down_out)))
    ]
    for m in served:
        m.start()

    for q in range(2):
        for k in NEAR:
            along(q, k, 1 - k % 2).wait_recv()
            along(q, k, 2).wait_recv()
    for k in FARS[:-1]:
        across(2, k).wait_recv()

    def near(k):
        return rem(y + 1 + 2 * rem(k, 2), NY)

    def other(k):
        return rem(y + 3 - 2 * rem(k, 2), NY)

    def far(n, k):
        return send(ps[n].at[k, far_y], rs_[n].at[k], fs.at[n, k], fr.at[n, k], at(g, z, near(k), t))

    def plain(n, k):
        return send(ps[n].at[k, other(k)], us_[n].at[k], us.at[n, k], ur.at[n, k], at(g, z, other(k), t))

    def summed(n, k):
        return send(as_[n].at[k], ws_[n].at[k], ws.at[n, k], wr.at[n, k], at(g, z, near(k), t))

    def back(n, k):
        src, dst = (os_[n].at[k], es[n].at[k]) if n < 2 else (pl_ref.at[k], el_ref.at[k])
        return send(src, dst, bs.at[n, k], br.at[n, k], at(g, z, y, rem(t + k, NT)))

    def experts(k):
        b = rem(t + k, NT)
        rows = jnp.concatenate(
            [x_ref[zi, b, yi] for zi in range(NZ) for yi in range(NY)],
            axis=1,
        )
        wide = rows.astype(F32)
        scale = lax.rsqrt(jnp.sum(wide * wide, axis=1, keepdims=True) / MODEL + norm_eps)
        rows = (wide * scale).astype(BF)
        dims = (((1,), (1,)), ((), ()))
        gate = lax.dot_general(rows, gate_ref[...], dims, preferred_element_type=F32)
        up = lax.dot_general(rows, up_ref[...], dims, preferred_element_type=F32)
        h_ref[k] = (gate / (1.0 + jnp.exp(-gate)) * up).astype(BF)

    def product(zi, k):
        cols = slice(zi * NY * FEAT, (zi + 1) * NY * FEAT)
        return jnp.dot(h_ref[k], down_ref[:, cols], preferred_element_type=F32).astype(BF)

    def products(n, k):
        for i, zi in enumerate(PARTS[n]):
            part = product(zi, k)
            for yi in range(NY):
                ps[n][k, yi, :, i * FEAT:(i + 1) * FEAT] = part[:, yi * FEAT:(yi + 1) * FEAT]

    def kth(i):
        return 4 + (1 - 2 * rem(i, 2)) * lax.div(i + 1, 2)

    def sweep0(i, _):
        k = kth(i)
        experts(k)
        products(0, k)
        late = product(LATE, k)
        far(0, k).start()
        plain(0, k).start()

        @pl.when(k > 0)
        def _():
            pl_ref[k] = late
            back(2, k).start()

        @pl.when(k == 0)
        def _():
            el_ref[k] = late

        return 0

    def relay(n, k):
        far(n, k).wait_recv()
        as_[n][k] = (rs_[n][k].astype(F32) + ps[n][k, near(k)].astype(F32)).astype(BF)
        summed(n, k).start()

    def finish(n, k):
        plain(n, k).wait_recv()
        summed(n, k).wait_recv()
        total = (ps[n][k, y].astype(F32) + us_[n][k].astype(F32) + ws_[n][k].astype(F32)).astype(BF)

        @pl.when(k > 0)
        def _():
            os_[n][k] = total
            back(n, k).start()

        @pl.when(k == 0)
        def _():
            es[n][k] = total

    def sweep1(i, _):
        k = kth(i)
        relay(0, k)
        products(1, k)
        far(1, k).start()
        plain(1, k).start()
        return 0

    def sweep2(i, _):
        k = kth(i)
        relay(1, k)
        finish(0, k)
        return 0

    def sweep3(i, _):
        finish(1, kth(i))
        return 0

    def combined(n):
        rows = es[n] if n < 2 else el_ref
        total = jnp.zeros((TOK, rows.shape[-1]), F32)
        for k in FARS:
            if k:
                back(n, k).wait_recv()
            for i in range(2):
                total = total + jnp.dot(comb_ref[k, i], rows[k], preferred_element_type=F32)
        return total

    def token_sum(i):
        to = rem(y + i, NY)
        return send(my_ref.at[to], ly_ref.at[y], ds.at[i], dr.at[i], at(g, z, to, t))

    def part(zi, zo):
        return send(m_ref.at[zo], l_ref.at[zi], cs.at[zo], cr.at[zi], at(g, zo, y, t))

    def home(zo):
        @pl.when(zo != z)
        def _():
            part(z, zo).start()

    def combine(n):
        total = combined(n)
        for i, zo in enumerate(PARTS[n]):
            m_ref[zo] = total[:, i * FEAT:(i + 1) * FEAT].astype(BF)
        for zo in PARTS[n]:
            home(zo)

    lax.fori_loop(0, NT, sweep0, 0)
    lax.fori_loop(0, NT, sweep1, 0)
    total = combined(2)
    for i in range(NY):
        my_ref[i] = total[:, i * FEAT:(i + 1) * FEAT].astype(BF)
    for i in (1, 3, 2):
        token_sum(i).start()
    lax.fori_loop(0, NT, sweep2, 0)
    combine(0)
    ly_ref[y] = my_ref[y]
    for i in (1, 3, 2):
        token_sum(i).wait_recv()
    total = jnp.zeros((TOK, FEAT), F32)
    for i in range(NY):
        total = total + ly_ref[i].astype(F32)
    m_ref[LATE] = total.astype(BF)
    home(LATE)
    lax.fori_loop(0, NT, sweep3, 0)
    combine(1)

    l_ref[z] = m_ref[z]
    own = jnp.zeros((TOK, FEAT), F32)
    for zi in range(NZ):
        @pl.when(zi != z)
        def _():
            part(zi, z).wait_recv()
    for zi in range(NZ):
        own = own + l_ref[zi].astype(F32)
    out_ref[...] = own.astype(BF)

    for m in served:
        m.wait()
    for i in (1, 2, 3):
        tok_copy(i).wait_send()
        tok_along(i).wait_send()
        token_sum(i).wait_send()
    for k in range(NT):
        for h in range(2):
            if k:
                first(k, h).wait_send()
            else:
                @pl.when(NC * c + h != y)
                def _():
                    first(k, h).wait_send()
    for j in range(NZ):
        for q in range(2):
            if j or q:
                second(j, q).wait_send()
    for k in range(1, NT):
        across(2, k).wait_send()
        back(2, k).wait_send()
    for n in range(2):
        for k in range(NT):
            for way in range(3):
                along(n, k, way).wait_send()
            if k:
                across(n, k).wait_send()
                back(n, k).wait_send()
            far(n, k).wait_send()
            plain(n, k).wait_send()
            summed(n, k).wait_send()
    for zo in range(NZ):
        @pl.when(zo != z)
        def _():
            part(z, zo).wait_send()


def hand_over(*refs):
    src, dst, held, ins, outs = refs[:4], refs[4:8], refs[8:12], refs[12], refs[13]
    reads = [pltpu.make_async_copy(src[i], held[i], ins.at[i]) for i in range(4)]
    writes = [pltpu.make_async_copy(held[i], dst[i], outs.at[i]) for i in range(4)]
    for r in reads:
        r.start()
    for r, w in zip(reads, writes):
        r.wait()
        w.start()
    for w in writes:
        w.wait()


def local(tokens, routes, route_weight, norm_gain, gate_master, up_master, down_master):
    vm = pl.BlockSpec(memory_space=pltpu.VMEM)
    any_ = pl.BlockSpec(memory_space=pl.ANY)
    dma = pltpu.SemaphoreType.DMA
    serving = jax.ShapeDtypeStruct((1, COLS, MODEL), BF)
    mixed = jax.ShapeDtypeStruct((TOK, FEAT), BF)
    master = pltpu.VMEM((EXPERTS, ROWS, WIDTH), F32)

    def rows(*dims):
        return pltpu.VMEM((*dims[:-1], CAP, dims[-1]), BF)

    def summing(width):
        return [rows(NT, NY, width)] + [rows(NT, width)] * 6

    shapes = (mixed, serving, serving, serving)
    results = pl.pallas_call(
        kernel,
        out_shape=shapes,
        in_specs=[vm, vm, vm, vm, any_, any_, any_],
        out_specs=(vm, any_, any_, any_),
        scratch_shapes=[
            master, master, master,
            pltpu.VMEM((16, TOK), F32),
            pltpu.VMEM((16, TOK), F32),
            pltpu.VMEM((NT, CAP, TOK), BF),
            pltpu.VMEM((NT, 2, TOK, CAP), BF),
            pltpu.VMEM((NT, 2, PACK, LANES), BF),
            pltpu.VMEM((NX, NY, PACK, LANES), BF),
            pltpu.VMEM((2 * NZ, NY, PACK, LANES), BF),
            pltpu.VMEM((NZ, TOK, FEAT), BF),
            pltpu.VMEM((NY, TOK, FEAT), BF),
            rows(NT, FEAT), rows(NT, 2, FEAT), rows(NT, NY, FEAT),
            rows(NZ, NT, NY, FEAT),
            pltpu.VMEM((COLS, MODEL), BF),
            pltpu.VMEM((COLS, MODEL), BF),
            pltpu.VMEM((COLS, MODEL), BF),
            rows(NT, COLS),
            *summing(2 * FEAT), *summing(FEAT),
            rows(NT, NY * FEAT), rows(NT, NY * FEAT),
            pltpu.VMEM((NY, TOK, FEAT), BF),
            pltpu.VMEM((NY, TOK, FEAT), BF),
            pltpu.VMEM((NZ, TOK, FEAT), BF),
            pltpu.VMEM((NZ, TOK, FEAT), BF),
            dma((3,)), dma((NZ,)), dma((NZ,)), dma((NY,)), dma((NY,)),
            dma((NT, 2)), dma((NX * NY,)),
            dma((NZ, 2)), dma((NZ, 2)),
            dma((3, NT)), dma((3, NT)),
            dma((2, NT, 3)), dma((2, NT, 3)),
            dma((2, NT)), dma((2, NT)), dma((2, NT)), dma((2, NT)),
            dma((2, NT)), dma((2, NT)), dma((3, NT)), dma((3, NT)),
            dma((NY,)), dma((NY,)),
            dma((NZ,)), dma((NZ,)), dma((3,)),
        ],
        compiler_params=pltpu.CompilerParams(collective_id=0, has_side_effects=True, vmem_limit_bytes=VMEM_LIMIT),
        name="handover_kernel",
    )(tokens, routes.T, route_weight.T, norm_gain[None, :], gate_master, up_master, down_master)
    out, gate_t, up_t, down_t = pl.pallas_call(
        hand_over,
        out_shape=shapes,
        in_specs=[any_] * 4,
        out_specs=(any_,) * 4,
        scratch_shapes=[pltpu.VMEM(v.shape, BF) for v in shapes] + [dma((4,)), dma((4,))],
        name="output_kernel",
    )(*results)
    return out, jnp.swapaxes(gate_t, 1, 2), jnp.swapaxes(up_t, 1, 2), jnp.swapaxes(down_t, 1, 2)


def solution(mesh):
    placed = (
        P(("gr", "tp"), "fs"),
        P(("gr", "tp"), None),
        P(("gr", "tp"), None),
        P(("gr", "fs")),
        P(None, ("gr", "fs"), "tp"),
        P(None, ("gr", "fs"), "tp"),
        P(None, ("gr", "fs"), "tp"),
    )
    return jax.shard_map(
        local,
        mesh=mesh,
        in_specs=placed,
        out_specs=(
            P(("gr", "tp"), "fs"),
            P("tp", None, "fs"),
            P("tp", None, "fs"),
            P("tp", None, "fs"),
        ),
        check_vma=False,
    )
```

```python
import jax
import jax.numpy as jnp
from jax import lax
from jax.experimental import pallas as pl
from jax.experimental.pallas import tpu as pltpu
from jax.sharding import PartitionSpec as P

norm_eps = 1e-06
BF = jnp.bfloat16
F32 = jnp.float32
I32 = jnp.int32
MESH = pl.DeviceIdType.MESH
VMEM_LIMIT = 60 * 1024 * 1024

NY, NZ, NX, NC = 4, 4, 4, 2
NT = NX * NC
EXPERTS = 8
CAP = 192
ROWS = 64
WIDTH = 352
COLS = 176
LANES = 128
DLO, DHI = 96, 80
PACK = COLS + DLO
TOK = 512
FEAT = 128
MODEL = 2048
NEAR = (0, 1, 7, 2, 6, 3, 5, 4)
FARS = (4, 3, 5, 2, 6, 1, 7, 0)
PARTS = ((0, 3), (2,))
LATE = 1


def rem(a, n):
    return lax.rem(a, n)


def at(g, z, y, t):
    return (g, z * NY + y, t)


def send(src, dst, ss, rs, to):
    return pltpu.make_async_remote_copy(
        src_ref=src, dst_ref=dst, send_sem=ss, recv_sem=rs, device_id=to, device_id_type=MESH
    )


def kernel(
    tok_ref, routes_ref, weight_ref, gain_ref, gm_hbm, um_hbm, dm_hbm,
    out_ref, gate_out, up_out, down_out,
    gm_ref, um_ref, dm_ref, key_ref, mix_ref, table_ref, comb_ref,
    wp_ref, q_ref, v_ref, t_ref, ty_ref, s0_ref, s1_ref, s2_ref, x_ref, gate_ref, up_ref, down_ref, h_ref,
    p0, r0, a0, u0, w0, o0, e0, p1, r1, a1, u1, w1, o1, e1, pl_ref, el_ref, my_ref, ly_ref, m_ref, l_ref,
    ms, zs, zr, tys, tyr, qs, qr, vs, vr, xs, xr, ys, yr,
    fs, fr, us, ur, ws, wr, bs, br, ds, dr, cs, cr, outs,
):
    ps, rs_, as_, us_, ws_, os_, es = ((p0, p1), (r0, r1), (a0, a1), (u0, u1), (w0, w1), (o0, o1), (e0, e1))
    g, f, t = lax.axis_index("gr"), lax.axis_index("fs"), lax.axis_index("tp")
    z, y = lax.div(f, NY), rem(f, NY)
    x, c = lax.div(t, NC), rem(t, NC)
    up_y, dn_y, far_y = rem(y + 1, NY), rem(y + NY - 1, NY), rem(y + 2, NY)

    masters = [
        pltpu.make_async_copy(src, dst, ms.at[i])
        for i, (src, dst) in enumerate(((gm_hbm, gm_ref), (um_hbm, um_ref), (dm_hbm, dm_ref)))
    ]
    for m in masters:
        m.start()

    barrier = pltpu.get_barrier_semaphore()
    count = 0
    for dy in range(NY):
        for dt in range(NT):
            if dy or dt:
                pl.semaphore_signal(barrier, inc=1, device_id=at(g, z, rem(y + dy, NY), rem(t + dt, NT)), device_id_type=MESH)
                count += 1
    for dg in range(2):
        for dz in range(NZ):
            if dg or dz:
                pl.semaphore_signal(barrier, inc=1, device_id=at(rem(g + dg, 2), rem(z + dz, NZ), y, t), device_id_type=MESH)
                count += 1

    ex = lax.broadcasted_iota(I32, (16, TOK), 0)
    first_is, second_is = routes_ref[0:1, :] == ex, routes_ref[1:2, :] == ex
    named = first_is | second_is
    before = lax.broadcasted_iota(I32, (TOK, TOK), 0) < lax.broadcasted_iota(I32, (TOK, TOK), 1)
    rank = jnp.dot(
        jnp.where(named, 1.0, 0.0).astype(BF), jnp.where(before, 1.0, 0.0).astype(BF), preferred_element_type=F32
    )
    key_ref[...] = jnp.where(named, rank, -1.0)
    mix_ref[...] = jnp.where(first_is, weight_ref[0:1, :], 0.0) + jnp.where(second_is, weight_ref[1:2, :], 0.0)
    slot = lax.broadcasted_iota(I32, (CAP, TOK), 0).astype(F32)

    def tables(k, _):
        key = key_ref[pl.ds(rem(t + k, NT), 1), :]
        table_ref[k] = jnp.where(slot == key, 1.0, 0.0).astype(BF)
        return 0

    lax.fori_loop(0, NT, tables, 0)
    ty_ref[y] = tok_ref[...]

    def weighting(k, _):
        e = rem(t + NT - k, NT)
        here = slot == key_ref[pl.ds(e, 1), :]
        mix = mix_ref[pl.ds(e, 1), :]
        high = mix.astype(BF).astype(F32)
        for i, part in enumerate((high, mix - high)):
            comb_ref[k, i] = jnp.transpose(jnp.where(here, part, 0.0)).astype(BF)
        return 0

    lax.fori_loop(0, NT, weighting, 0)

    for m in masters:
        m.wait()
    gain = jnp.concatenate([gain_ref[...], gain_ref[...]], axis=1)

    def pack(e, _):
        pad = jnp.zeros((2 * ROWS, 3 * LANES - WIDTH), F32)
        gu = jnp.concatenate([gm_ref[e], um_ref[e]], axis=0)
        gu = (jnp.transpose(jnp.concatenate([gu, pad], axis=1)) * gain).astype(BF)
        dn = dm_ref[e]
        dn = jnp.concatenate([dn, pad[:ROWS]], axis=1)
        dd = jnp.concatenate([dn, pltpu.roll(dn, 3 * LANES - DLO, 1)], axis=0)
        dd = jnp.transpose(dd).astype(BF)
        for h in range(2):
            lo = h * COLS
            wp_ref[e, h, 0:COLS, :] = gu[lo:lo + COLS]
            wp_ref[e, h, COLS:PACK, :] = dd[lo:lo + DLO]

        return 0

    lax.fori_loop(0, NT, pack, 0)
    pl.semaphore_wait(barrier, count)

    low, base = rem(z, 2), 2 * lax.div(z, 2)
    peers = {1: base + 1 - low, 2: 2 - base + low, 3: 3 - base - low}

    def tok_copy(i):
        return send(tok_ref, t_ref.at[z], zs.at[i], zr.at[i], at(g, peers[i], y, t))

    def tok_along(i):
        return send(tok_ref, ty_ref.at[y], tys.at[i], tyr.at[i], at(g, z, rem(y + i, NY), t))

    for i in (1, 2, 3):
        tok_copy(i).start()
    def first(e, h):
        return send(
            wp_ref.at[e, h], q_ref.at[x, y], qs.at[e, h], qr.at[x * NY + y], at(g, z, NC * c + h, e)
        )

    def stays(e, h):
        return (NC * c + h == y) & (e == t)

    for i in range(NX):
        for n in range(NC):
            e = NC * rem(x + 2 * NX - z - i, NX) + n
            for h in range(2):
                @pl.when(stays(e, h))
                def _():
                    pltpu.make_async_copy(wp_ref.at[e, h], q_ref.at[x, y], qr.at[x * NY + y]).start()

                @pl.when(jnp.logical_not(stays(e, h)))
                def _():
                    first(e, h).start()

    for i in (1, 3, 2):
        tok_along(i).start()

    mate, rest = peers[1], 2 - base
    tiles = (mate, pl.ds(rest, 2))
    stage = (s0_ref, s1_ref)

    def dispatch(q):
        rows_in = t_ref[mate] if q == 0 else jnp.concatenate([t_ref[rest], t_ref[rest + 1]], axis=1)
        for k in NEAR:
            rows = jnp.dot(table_ref[k], rows_in, preferred_element_type=F32).astype(BF)
            for i in range(1 + q):
                part = rows[:, i * FEAT:(i + 1) * FEAT]
                if k == 0:
                    x_ref[rest + i if q else mate, t, y] = part
                elif q:
                    s1_ref[k, i] = part
                else:
                    s0_ref[k] = part

    def dispatch_own():
        rows_in = jnp.concatenate([ty_ref[i] for i in range(NY)], axis=1)
        for k in NEAR:
            rows = jnp.dot(table_ref[k], rows_in, preferred_element_type=F32).astype(BF)
            for i in range(NY):
                part = rows[:, i * FEAT:(i + 1) * FEAT]
                if k == 0:
                    x_ref[z, t, i] = part
                else:
                    s2_ref[k, i] = part

    def across(q, k):
        if q == 2:
            src, dst = s2_ref.at[k], x_ref.at[z, t]
        else:
            src, dst = stage[q].at[k], x_ref.at[tiles[q], t, y]
        return send(src, dst, xs.at[q, k], xr.at[q, k], at(g, z, y, rem(t + k, NT)))

    def along(q, k, way):
        b = rem(t + NT - k, NT)
        whose = y if way < 2 else (dn_y if k % 2 == 0 else up_y)
        to = up_y if way == 0 or (way == 2 and k % 2 == 0) else dn_y
        ref = x_ref.at[tiles[q], b, whose]
        return send(ref, ref, ys.at[q, k, way], yr.at[q, k, way], at(g, z, to, t))

    def spread(q, k):
        if k:
            across(q, k).wait_recv()
        along(q, k, 0).start()
        along(q, k, 1).start()

    def forward(q, k):
        along(q, k, k % 2).wait_recv()
        along(q, k, 2).start()

    zz = g * NZ + z

    def second(j, q):
        zd = rem(z + j, NZ)
        return send(q_ref.at[zd], v_ref.at[zz], vs.at[j, q], vr.at[j, q], at(rem(g + q, 2), zd, y, t))

    own_v = pltpu.make_async_copy(q_ref.at[z], v_ref.at[zz], vr.at[0, 0])

    def weights_on(i):
        zd = rem(x + z + i, NX)
        for n in range(NY):
            send(q_ref.at[zd, n], q_ref.at[zd, n], qs.at[0, 0], qr.at[zd * NY + n], at(g, z, up_y, t)).wait_recv()
        j = rem(zd + NZ - z, NZ)
        second(j, 1).start()

        @pl.when(j > 0)
        def _():
            second(j, 0).start()

        @pl.when(j == 0)
        def _():
            own_v.start()

    tok_copy(1).wait_recv()
    dispatch(0)
    for k in NEAR[1:]:
        across(0, k).start()
    spread(0, 0)
    weights_on(0)
    weights_on(1)
    tok_copy(2).wait_recv()
    tok_copy(3).wait_recv()
    dispatch(1)
    for k in NEAR[1:]:
        across(1, k).start()
    spread(1, 0)
    weights_on(2)
    weights_on(3)
    for k in NEAR[1:]:
        spread(0, k)
    for i in (1, 3, 2):
        tok_along(i).wait_recv()
    dispatch_own()
    for k in NEAR:
        forward(0, k)
        if k:
            spread(1, k)
    for k in FARS[:-1]:
        across(2, k).start()
    for k in NEAR:
        forward(1, k)

    left = lax.broadcasted_iota(I32, (COLS, LANES), 1) < ROWS

    def unpack(zs_):
        for i in range(NY // 2):
            a, b = (v_ref[zs_, 2 * i + n].astype(F32) for n in range(2))
            ra, rb = pltpu.roll(a, ROWS, 1), pltpu.roll(b, ROWS, 1)
            cols = pl.ds(pl.multiple_of((zs_ * (NY // 2) + i) * LANES, LANES), LANES)
            gate_ref[:, cols] = jnp.where(left, a[:COLS], rb[:COLS]).astype(BF)
            up_ref[:, cols] = jnp.where(left, ra[:COLS], b[:COLS]).astype(BF)
            down_ref[0:DLO, cols] = jnp.where(left[:DLO], a[COLS:], rb[COLS:]).astype(BF)
            down_ref[DLO:COLS, cols] = jnp.where(left[:DHI], ra[COLS:COLS + DHI], b[COLS:COLS + DHI]).astype(BF)

    own_v.wait()
    unpack(zz)
    for j, q in ((1, 0), (3, 0), (2, 0), (1, 1), (3, 1), (2, 1), (0, 1)):
        second(j, q).wait_recv()
        unpack(rem(g + q, 2) * NZ + rem(z + NZ - j, NZ))
    served = [
        pltpu.make_async_copy(src, dst.at[0], outs.at[i])
        for i, (src, dst) in enumerate(((gate_ref, gate_out), (up_ref, up_out), (down_ref, down_out)))
    ]
    for m in served:
        m.start()

    for q in range(2):
        for k in NEAR:
            along(q, k, 1 - k % 2).wait_recv()
            along(q, k, 2).wait_recv()
    for k in FARS[:-1]:
        across(2, k).wait_recv()

    def near(k):
        return rem(y + 1 + 2 * rem(k, 2), NY)

    def other(k):
        return rem(y + 3 - 2 * rem(k, 2), NY)

    def far(n, k):
        return send(ps[n].at[k, far_y], rs_[n].at[k], fs.at[n, k], fr.at[n, k], at(g, z, near(k), t))

    def plain(n, k):
        return send(ps[n].at[k, other(k)], us_[n].at[k], us.at[n, k], ur.at[n, k], at(g, z, other(k), t))

    def summed(n, k):
        return send(as_[n].at[k], ws_[n].at[k], ws.at[n, k], wr.at[n, k], at(g, z, near(k), t))

    def back(n, k):
        src, dst = (os_[n].at[k], es[n].at[k]) if n < 2 else (pl_ref.at[k], el_ref.at[k])
        return send(src, dst, bs.at[n, k], br.at[n, k], at(g, z, y, rem(t + k, NT)))

    def experts(k):
        b = rem(t + k, NT)
        rows = jnp.concatenate(
            [x_ref[zi, b, yi] for zi in range(NZ) for yi in range(NY)],
            axis=1,
        )
        wide = rows.astype(F32)
        scale = lax.rsqrt(jnp.sum(wide * wide, axis=1, keepdims=True) / MODEL + norm_eps)
        rows = (wide * scale).astype(BF)
        dims = (((1,), (1,)), ((), ()))
        gate = lax.dot_general(rows, gate_ref[...], dims, preferred_element_type=F32)
        up = lax.dot_general(rows, up_ref[...], dims, preferred_element_type=F32)
        h_ref[k] = (gate / (1.0 + jnp.exp(-gate)) * up).astype(BF)

    def product(zi, k):
        cols = slice(zi * NY * FEAT, (zi + 1) * NY * FEAT)
        return jnp.dot(h_ref[k], down_ref[:, cols], preferred_element_type=F32).astype(BF)

    def products(n, k):
        for i, zi in enumerate(PARTS[n]):
            part = product(zi, k)
            for yi in range(NY):
                ps[n][k, yi, :, i * FEAT:(i + 1) * FEAT] = part[:, yi * FEAT:(yi + 1) * FEAT]

    def kth(i):
        return 4 + (1 - 2 * rem(i, 2)) * lax.div(i + 1, 2)

    def sweep0(i, _):
        k = kth(i)
        experts(k)
        products(0, k)
        late = product(LATE, k)
        far(0, k).start()
        plain(0, k).start()

        @pl.when(k > 0)
        def _():
            pl_ref[k] = late
            back(2, k).start()

        @pl.when(k == 0)
        def _():
            el_ref[k] = late

        return 0

    def relay(n, k):
        far(n, k).wait_recv()
        as_[n][k] = (rs_[n][k].astype(F32) + ps[n][k, near(k)].astype(F32)).astype(BF)
        summed(n, k).start()

    def finish(n, k):
        plain(n, k).wait_recv()
        summed(n, k).wait_recv()
        total = (ps[n][k, y].astype(F32) + us_[n][k].astype(F32) + ws_[n][k].astype(F32)).astype(BF)

        @pl.when(k > 0)
        def _():
            os_[n][k] = total
            back(n, k).start()

        @pl.when(k == 0)
        def _():
            es[n][k] = total

    def sweep1(i, _):
        k = kth(i)
        relay(0, k)
        products(1, k)
        far(1, k).start()
        plain(1, k).start()
        return 0

    def sweep2(i, _):
        k = kth(i)
        relay(1, k)
        finish(0, k)
        return 0

    def sweep3(i, _):
        finish(1, kth(i))
        return 0

    def combined(n):
        rows = es[n] if n < 2 else el_ref
        total = jnp.zeros((TOK, rows.shape[-1]), F32)
        for k in FARS:
            if k:
                back(n, k).wait_recv()
            for i in range(2):
                total = total + jnp.dot(comb_ref[k, i], rows[k], preferred_element_type=F32)
        return total

    def token_sum(i):
        to = rem(y + i, NY)
        return send(my_ref.at[to], ly_ref.at[y], ds.at[i], dr.at[i], at(g, z, to, t))

    def part(zi, zo):
        return send(m_ref.at[zo], l_ref.at[zi], cs.at[zo], cr.at[zi], at(g, zo, y, t))

    def home(zo):
        @pl.when(zo != z)
        def _():
            part(z, zo).start()

    def combine(n):
        total = combined(n)
        for i, zo in enumerate(PARTS[n]):
            m_ref[zo] = total[:, i * FEAT:(i + 1) * FEAT].astype(BF)
        for zo in PARTS[n]:
            home(zo)

    lax.fori_loop(0, NT, sweep0, 0)
    lax.fori_loop(0, NT, sweep1, 0)
    total = combined(2)
    for i in range(NY):
        my_ref[i] = total[:, i * FEAT:(i + 1) * FEAT].astype(BF)
    for i in (1, 3, 2):
        token_sum(i).start()
    lax.fori_loop(0, NT, sweep2, 0)
    combine(0)
    ly_ref[y] = my_ref[y]
    for i in (1, 3, 2):
        token_sum(i).wait_recv()
    total = jnp.zeros((TOK, FEAT), F32)
    for i in range(NY):
        total = total + ly_ref[i].astype(F32)
    m_ref[LATE] = total.astype(BF)
    home(LATE)
    lax.fori_loop(0, NT, sweep3, 0)
    combine(1)

    l_ref[z] = m_ref[z]
    own = jnp.zeros((TOK, FEAT), F32)
    for zi in range(NZ):
        @pl.when(zi != z)
        def _():
            part(zi, z).wait_recv()
    for zi in range(NZ):
        own = own + l_ref[zi].astype(F32)
    out_ref[...] = own.astype(BF)

    for m in served:
        m.wait()
    for i in (1, 2, 3):
        tok_copy(i).wait_send()
        tok_along(i).wait_send()
        token_sum(i).wait_send()
    for e in range(NT):
        for h in range(2):
            @pl.when(jnp.logical_not(stays(e, h)))
            def _():
                first(e, h).wait_send()
    for j in range(NZ):
        for q in range(2):
            if j or q:
                second(j, q).wait_send()
    for k in range(1, NT):
        across(2, k).wait_send()
        back(2, k).wait_send()
    for n in range(2):
        for k in range(NT):
            for way in range(3):
                along(n, k, way).wait_send()
            if k:
                across(n, k).wait_send()
                back(n, k).wait_send()
            far(n, k).wait_send()
            plain(n, k).wait_send()
            summed(n, k).wait_send()
    for zo in range(NZ):
        @pl.when(zo != z)
        def _():
            part(z, zo).wait_send()


def hand_over(*refs):
    src, dst, held, ins, outs = refs[:4], refs[4:8], refs[8:12], refs[12], refs[13]
    reads = [pltpu.make_async_copy(src[i], held[i], ins.at[i]) for i in range(4)]
    writes = [pltpu.make_async_copy(held[i], dst[i], outs.at[i]) for i in range(4)]
    for r in reads:
        r.start()
    for r, w in zip(reads, writes):
        r.wait()
        w.start()
    for w in writes:
        w.wait()


def local(tokens, routes, route_weight, norm_gain, gate_master, up_master, down_master):
    vm = pl.BlockSpec(memory_space=pltpu.VMEM)
    any_ = pl.BlockSpec(memory_space=pl.ANY)
    dma = pltpu.SemaphoreType.DMA
    serving = jax.ShapeDtypeStruct((1, COLS, MODEL), BF)
    mixed = jax.ShapeDtypeStruct((TOK, FEAT), BF)
    master = pltpu.VMEM((EXPERTS, ROWS, WIDTH), F32)

    def rows(*dims):
        return pltpu.VMEM((*dims[:-1], CAP, dims[-1]), BF)

    def summing(width):
        return [rows(NT, NY, width)] + [rows(NT, width)] * 6

    shapes = (mixed, serving, serving, serving)
    results = pl.pallas_call(
        kernel,
        out_shape=shapes,
        in_specs=[vm, vm, vm, vm, any_, any_, any_],
        out_specs=(vm, any_, any_, any_),
        scratch_shapes=[
            master, master, master,
            pltpu.VMEM((16, TOK), F32),
            pltpu.VMEM((16, TOK), F32),
            pltpu.VMEM((NT, CAP, TOK), BF),
            pltpu.VMEM((NT, 2, TOK, CAP), BF),
            pltpu.VMEM((NT, 2, PACK, LANES), BF),
            pltpu.VMEM((NX, NY, PACK, LANES), BF),
            pltpu.VMEM((2 * NZ, NY, PACK, LANES), BF),
            pltpu.VMEM((NZ, TOK, FEAT), BF),
            pltpu.VMEM((NY, TOK, FEAT), BF),
            rows(NT, FEAT), rows(NT, 2, FEAT), rows(NT, NY, FEAT),
            rows(NZ, NT, NY, FEAT),
            pltpu.VMEM((COLS, MODEL), BF),
            pltpu.VMEM((COLS, MODEL), BF),
            pltpu.VMEM((COLS, MODEL), BF),
            rows(NT, COLS),
            *summing(2 * FEAT), *summing(FEAT),
            rows(NT, NY * FEAT), rows(NT, NY * FEAT),
            pltpu.VMEM((NY, TOK, FEAT), BF),
            pltpu.VMEM((NY, TOK, FEAT), BF),
            pltpu.VMEM((NZ, TOK, FEAT), BF),
            pltpu.VMEM((NZ, TOK, FEAT), BF),
            dma((3,)), dma((NZ,)), dma((NZ,)), dma((NY,)), dma((NY,)),
            dma((NT, 2)), dma((NX * NY,)),
            dma((NZ, 2)), dma((NZ, 2)),
            dma((3, NT)), dma((3, NT)),
            dma((2, NT, 3)), dma((2, NT, 3)),
            dma((2, NT)), dma((2, NT)), dma((2, NT)), dma((2, NT)),
            dma((2, NT)), dma((2, NT)), dma((3, NT)), dma((3, NT)),
            dma((NY,)), dma((NY,)),
            dma((NZ,)), dma((NZ,)), dma((3,)),
        ],
        compiler_params=pltpu.CompilerParams(collective_id=0, has_side_effects=True, vmem_limit_bytes=VMEM_LIMIT),
        name="handover_kernel",
    )(tokens, routes.T, route_weight.T, norm_gain[None, :], gate_master, up_master, down_master)
    out, gate_t, up_t, down_t = pl.pallas_call(
        hand_over,
        out_shape=shapes,
        in_specs=[any_] * 4,
        out_specs=(any_,) * 4,
        scratch_shapes=[pltpu.VMEM(v.shape, BF) for v in shapes] + [dma((4,)), dma((4,))],
        name="output_kernel",
    )(*results)
    return out, jnp.swapaxes(gate_t, 1, 2), jnp.swapaxes(up_t, 1, 2), jnp.swapaxes(down_t, 1, 2)


def solution(mesh):
    placed = (
        P(("gr", "tp"), "fs"),
        P(("gr", "tp"), None),
        P(("gr", "tp"), None),
        P(("gr", "fs")),
        P(None, ("gr", "fs"), "tp"),
        P(None, ("gr", "fs"), "tp"),
        P(None, ("gr", "fs"), "tp"),
    )
    return jax.shard_map(
        local,
        mesh=mesh,
        in_specs=placed,
        out_specs=(
            P(("gr", "tp"), "fs"),
            P("tp", None, "fs"),
            P("tp", None, "fs"),
            P("tp", None, "fs"),
        ),
        check_vma=False,
    )
```

```python
import jax
import jax.numpy as jnp
from jax import lax
from jax.experimental import pallas as pl
from jax.experimental.pallas import tpu as pltpu
from jax.sharding import PartitionSpec as P

norm_eps = 1e-06
BF = jnp.bfloat16
F32 = jnp.float32
I32 = jnp.int32
MESH = pl.DeviceIdType.MESH
VMEM_LIMIT = 60 * 1024 * 1024

NY, NZ, NX, NC = 4, 4, 4, 2
NT = NX * NC
EXPERTS = 8
CAP = 192
ROWS = 64
WIDTH = 352
COLS = 176
LANES = 128
DOWN = COLS // 2
PACK = COLS + DOWN
TOK = 512
FEAT = 128
MODEL = 2048
NEAR = (0, 1, 7, 2, 6, 3, 5, 4)
FARS = (4, 3, 5, 2, 6, 1, 7, 0)
PARTS = ((0, 3), (2,))
LATE = 1


def rem(a, n):
    return lax.rem(a, n)


def at(g, z, y, t):
    return (g, z * NY + y, t)


def send(src, dst, ss, rs, to):
    return pltpu.make_async_remote_copy(
        src_ref=src, dst_ref=dst, send_sem=ss, recv_sem=rs, device_id=to, device_id_type=MESH
    )


def kernel(
    tok_ref, routes_ref, weight_ref, gain_ref, gm_hbm, um_hbm, dm_hbm,
    out_ref, gate_out, up_out, down_out,
    gm_ref, um_ref, dm_ref, key_ref, mix_ref, table_ref, comb_ref,
    wp_ref, q_ref, v_ref, t_ref, ty_ref, s0_ref, s1_ref, s2_ref, x_ref, gate_ref, up_ref, down_ref, h_ref,
    p0, r0, a0, u0, w0, o0, e0, p1, r1, a1, u1, w1, o1, e1, pl_ref, el_ref, my_ref, ly_ref, m_ref, l_ref,
    ms, zs, zr, tys, tyr, qs, qr, vs, vr, xs, xr, ys, yr,
    fs, fr, us, ur, ws, wr, bs, br, ds, dr, cs, cr, outs,
):
    ps, rs_, as_, us_, ws_, os_, es = ((p0, p1), (r0, r1), (a0, a1), (u0, u1), (w0, w1), (o0, o1), (e0, e1))
    g, f, t = lax.axis_index("gr"), lax.axis_index("fs"), lax.axis_index("tp")
    z, y = lax.div(f, NY), rem(f, NY)
    x, c = lax.div(t, NC), rem(t, NC)
    up_y, dn_y, far_y = rem(y + 1, NY), rem(y + NY - 1, NY), rem(y + 2, NY)

    masters = [
        pltpu.make_async_copy(src, dst, ms.at[i])
        for i, (src, dst) in enumerate(((gm_hbm, gm_ref), (um_hbm, um_ref), (dm_hbm, dm_ref)))
    ]
    for m in masters:
        m.start()

    barrier = pltpu.get_barrier_semaphore()
    count = 0
    for dy in range(NY):
        for dt in range(NT):
            if dy or dt:
                pl.semaphore_signal(barrier, inc=1, device_id=at(g, z, rem(y + dy, NY), rem(t + dt, NT)), device_id_type=MESH)
                count += 1
    for dg in range(2):
        for dz in range(NZ):
            if dg or dz:
                pl.semaphore_signal(barrier, inc=1, device_id=at(rem(g + dg, 2), rem(z + dz, NZ), y, t), device_id_type=MESH)
                count += 1

    ex = lax.broadcasted_iota(I32, (16, TOK), 0)
    first_is, second_is = routes_ref[0:1, :] == ex, routes_ref[1:2, :] == ex
    named = first_is | second_is
    before = lax.broadcasted_iota(I32, (TOK, TOK), 0) < lax.broadcasted_iota(I32, (TOK, TOK), 1)
    rank = jnp.dot(
        jnp.where(named, 1.0, 0.0).astype(BF), jnp.where(before, 1.0, 0.0).astype(BF), preferred_element_type=F32
    )
    key_ref[...] = jnp.where(named, rank, -1.0)
    mix_ref[...] = jnp.where(first_is, weight_ref[0:1, :], 0.0) + jnp.where(second_is, weight_ref[1:2, :], 0.0)
    slot = lax.broadcasted_iota(I32, (CAP, TOK), 0).astype(F32)

    def tables(k, _):
        key = key_ref[pl.ds(rem(t + k, NT), 1), :]
        table_ref[k] = jnp.where(slot == key, 1.0, 0.0).astype(BF)
        return 0

    lax.fori_loop(0, NT, tables, 0)
    ty_ref[y] = tok_ref[...]

    def weighting(k, _):
        e = rem(t + NT - k, NT)
        here = slot == key_ref[pl.ds(e, 1), :]
        mix = mix_ref[pl.ds(e, 1), :]
        high = mix.astype(BF).astype(F32)
        for i, part in enumerate((high, mix - high)):
            comb_ref[k, i] = jnp.transpose(jnp.where(here, part, 0.0)).astype(BF)
        return 0

    lax.fori_loop(0, NT, weighting, 0)

    for m in masters:
        m.wait()
    gain = jnp.concatenate([gain_ref[...], gain_ref[...]], axis=1)

    def pack(e, _):
        pad = jnp.zeros((2 * ROWS, 3 * LANES - WIDTH), F32)
        gu = jnp.concatenate([gm_ref[e], um_ref[e]], axis=0)
        gu = jnp.transpose(jnp.concatenate([gu, pad], axis=1)) * gain
        dn = dm_ref[e]
        dn = jnp.concatenate([dn, pad[:ROWS]], axis=1)
        dd = jnp.concatenate([dn, pltpu.roll(dn, 3 * LANES - DOWN, 1)], axis=0)
        dd = jnp.transpose(dd)
        for h in range(2):
            lo = h * COLS
            wp_ref[e, h] = jnp.concatenate([gu[lo:lo + COLS], dd[lo:lo + DOWN]], axis=0).astype(BF)

        return 0

    lax.fori_loop(0, NT, pack, 0)
    pl.semaphore_wait(barrier, count)

    low, base = rem(z, 2), 2 * lax.div(z, 2)
    peers = {1: base + 1 - low, 2: 2 - base + low, 3: 3 - base - low}

    def tok_copy(i):
        return send(tok_ref, t_ref.at[z], zs.at[i], zr.at[i], at(g, peers[i], y, t))

    def tok_along(i):
        return send(tok_ref, ty_ref.at[y], tys.at[i], tyr.at[i], at(g, z, rem(y + i, NY), t))

    for i in (1, 2, 3):
        tok_copy(i).start()
    def first(e, h):
        return send(
            wp_ref.at[e, h], q_ref.at[x, y], qs.at[e, h], qr.at[x * NY + y], at(g, z, NC * c + h, e)
        )

    def stays(e, h):
        return (NC * c + h == y) & (e == t)

    def pieces(i):
        return [(NC * rem(x + 2 * NX - z - i, NX) + n, h) for n in range(NC) for h in range(2)]

    def wave(i):
        for e, h in pieces(i):
            @pl.when(stays(e, h))
            def _():
                pltpu.make_async_copy(wp_ref.at[e, h], q_ref.at[x, y], qr.at[x * NY + y]).start()

            @pl.when(jnp.logical_not(stays(e, h)))
            def _():
                first(e, h).start()

    def wave_left(i):
        for e, h in pieces(i):
            @pl.when(jnp.logical_not(stays(e, h)))
            def _():
                first(e, h).wait_send()

    wave(0)
    wave(1)


    mate, rest = peers[1], 2 - base
    tiles = (mate, pl.ds(rest, 2))
    stage = (s0_ref, s1_ref)

    def dispatch(q):
        rows_in = t_ref[mate] if q == 0 else jnp.concatenate([t_ref[rest], t_ref[rest + 1]], axis=1)
        for k in NEAR:
            rows = jnp.dot(table_ref[k], rows_in, preferred_element_type=F32).astype(BF)
            for i in range(1 + q):
                part = rows[:, i * FEAT:(i + 1) * FEAT]
                if k == 0:
                    x_ref[rest + i if q else mate, t, y] = part
                elif q:
                    s1_ref[k, i] = part
                else:
                    s0_ref[k] = part

    def dispatch_own():
        rows_in = jnp.concatenate([ty_ref[i] for i in range(NY)], axis=1)
        for k in NEAR:
            rows = jnp.dot(table_ref[k], rows_in, preferred_element_type=F32).astype(BF)
            for i in range(NY):
                part = rows[:, i * FEAT:(i + 1) * FEAT]
                if k == 0:
                    x_ref[z, t, i] = part
                else:
                    s2_ref[k, i] = part

    def across(q, k):
        if q == 2:
            src, dst = s2_ref.at[k], x_ref.at[z, t]
        else:
            src, dst = stage[q].at[k], x_ref.at[tiles[q], t, y]
        return send(src, dst, xs.at[q, k], xr.at[q, k], at(g, z, y, rem(t + k, NT)))

    def along(q, k, way):
        b = rem(t + NT - k, NT)
        whose = y if way < 2 else (dn_y if k % 2 == 0 else up_y)
        to = up_y if way == 0 or (way == 2 and k % 2 == 0) else dn_y
        ref = x_ref.at[tiles[q], b, whose]
        return send(ref, ref, ys.at[q, k, way], yr.at[q, k, way], at(g, z, to, t))

    def spread(q, k):
        if k:
            across(q, k).wait_recv()
        along(q, k, 0).start()
        along(q, k, 1).start()

    def forward(q, k):
        along(q, k, k % 2).wait_recv()
        along(q, k, 2).start()

    zz = g * NZ + z

    def second(j, q):
        zd = rem(z + j, NZ)
        return send(q_ref.at[zd], v_ref.at[zz], vs.at[j, q], vr.at[j, q], at(rem(g + q, 2), zd, y, t))

    own_v = pltpu.make_async_copy(q_ref.at[z], v_ref.at[zz], vr.at[0, 0])

    def weights_on(i):
        zd = rem(x + z + i, NX)
        for n in range(NY):
            send(q_ref.at[zd, n], q_ref.at[zd, n], qs.at[0, 0], qr.at[zd * NY + n], at(g, z, up_y, t)).wait_recv()
        j = rem(zd + NZ - z, NZ)
        second(j, 1).start()

        @pl.when(j > 0)
        def _():
            second(j, 0).start()

        @pl.when(j == 0)
        def _():
            own_v.start()

    tok_copy(1).wait_recv()
    dispatch(0)
    for k in NEAR[1:]:
        across(0, k).start()
    spread(0, 0)
    wave_left(0)
    wave(2)
    weights_on(0)
    wave_left(1)
    wave(3)
    for i in (1, 3, 2):
        tok_along(i).start()
    weights_on(1)
    tok_copy(2).wait_recv()
    tok_copy(3).wait_recv()
    dispatch(1)
    for k in NEAR[1:]:
        across(1, k).start()
    spread(1, 0)
    weights_on(2)
    weights_on(3)
    for k in NEAR[1:]:
        spread(0, k)
    for i in (1, 3, 2):
        tok_along(i).wait_recv()
    dispatch_own()
    for k in NEAR:
        forward(0, k)
        if k:
            spread(1, k)
    for k in FARS[:-1]:
        across(2, k).start()
    for k in NEAR:
        forward(1, k)

    left = lax.broadcasted_iota(I32, (COLS, LANES), 1) < ROWS

    def unpack(zs_):
        for i in range(NY // 2):
            a, b = (v_ref[zs_, 2 * i + n].astype(F32) for n in range(2))
            ra, rb = pltpu.roll(a, ROWS, 1), pltpu.roll(b, ROWS, 1)
            cols = pl.ds(pl.multiple_of((zs_ * (NY // 2) + i) * LANES, LANES), LANES)
            gate_ref[:, cols] = jnp.where(left, a[:COLS], rb[:COLS]).astype(BF)
            up_ref[:, cols] = jnp.where(left, ra[:COLS], b[:COLS]).astype(BF)
            down_ref[:, cols] = jnp.concatenate(
                [jnp.where(left[:DOWN], a[COLS:], rb[COLS:]), jnp.where(left[:DOWN], ra[COLS:], b[COLS:])], axis=0
            ).astype(BF)

    own_v.wait()
    unpack(zz)
    for j, q in ((1, 0), (3, 0), (2, 0), (1, 1), (3, 1), (2, 1), (0, 1)):
        second(j, q).wait_recv()
        unpack(rem(g + q, 2) * NZ + rem(z + NZ - j, NZ))
    served = [
        pltpu.make_async_copy(src, dst.at[0], outs.at[i])
        for i, (src, dst) in enumerate(((gate_ref, gate_out), (up_ref, up_out), (down_ref, down_out)))
    ]
    for m in served:
        m.start()

    for q in range(2):
        for k in NEAR:
            along(q, k, 1 - k % 2).wait_recv()
            along(q, k, 2).wait_recv()
    for k in FARS[:-1]:
        across(2, k).wait_recv()

    def near(k):
        return rem(y + 1 + 2 * rem(k, 2), NY)

    def other(k):
        return rem(y + 3 - 2 * rem(k, 2), NY)

    def far(n, k):
        return send(ps[n].at[k, far_y], rs_[n].at[k], fs.at[n, k], fr.at[n, k], at(g, z, near(k), t))

    def plain(n, k):
        return send(ps[n].at[k, other(k)], us_[n].at[k], us.at[n, k], ur.at[n, k], at(g, z, other(k), t))

    def summed(n, k):
        return send(as_[n].at[k], ws_[n].at[k], ws.at[n, k], wr.at[n, k], at(g, z, near(k), t))

    def back(n, k):
        src, dst = (os_[n].at[k], es[n].at[k]) if n < 2 else (pl_ref.at[k], el_ref.at[k])
        return send(src, dst, bs.at[n, k], br.at[n, k], at(g, z, y, rem(t + k, NT)))

    def experts(k):
        b = rem(t + k, NT)
        rows = jnp.concatenate(
            [x_ref[zi, b, yi] for zi in range(NZ) for yi in range(NY)],
            axis=1,
        )
        wide = rows.astype(F32)
        scale = lax.rsqrt(jnp.sum(wide * wide, axis=1, keepdims=True) / MODEL + norm_eps)
        rows = (wide * scale).astype(BF)
        dims = (((1,), (1,)), ((), ()))
        gate = lax.dot_general(rows, gate_ref[...], dims, preferred_element_type=F32)
        up = lax.dot_general(rows, up_ref[...], dims, preferred_element_type=F32)
        h_ref[k] = (gate / (1.0 + jnp.exp(-gate)) * up).astype(BF)

    def product(zi, k):
        cols = slice(zi * NY * FEAT, (zi + 1) * NY * FEAT)
        return jnp.dot(h_ref[k], down_ref[:, cols], preferred_element_type=F32).astype(BF)

    def products(n, k):
        for i, zi in enumerate(PARTS[n]):
            part = product(zi, k)
            for yi in range(NY):
                ps[n][k, yi, :, i * FEAT:(i + 1) * FEAT] = part[:, yi * FEAT:(yi + 1) * FEAT]

    def kth(i):
        return 4 + (1 - 2 * rem(i, 2)) * lax.div(i + 1, 2)

    def sweep0(i, _):
        k = kth(i)
        experts(k)
        products(0, k)
        late = product(LATE, k)
        far(0, k).start()
        plain(0, k).start()

        @pl.when(k > 0)
        def _():
            pl_ref[k] = late
            back(2, k).start()

        @pl.when(k == 0)
        def _():
            el_ref[k] = late

        return 0

    def relay(n, k):
        far(n, k).wait_recv()
        as_[n][k] = (rs_[n][k].astype(F32) + ps[n][k, near(k)].astype(F32)).astype(BF)
        summed(n, k).start()

    def finish(n, k):
        plain(n, k).wait_recv()
        summed(n, k).wait_recv()
        total = (ps[n][k, y].astype(F32) + us_[n][k].astype(F32) + ws_[n][k].astype(F32)).astype(BF)

        @pl.when(k > 0)
        def _():
            os_[n][k] = total
            back(n, k).start()

        @pl.when(k == 0)
        def _():
            es[n][k] = total

    def sweep1(i, _):
        k = kth(i)
        relay(0, k)
        products(1, k)
        far(1, k).start()
        plain(1, k).start()
        return 0

    def sweep2(i, _):
        k = kth(i)
        relay(1, k)
        finish(0, k)
        return 0

    def sweep3(i, _):
        finish(1, kth(i))
        return 0

    def combined(n):
        rows = es[n] if n < 2 else el_ref
        total = jnp.zeros((TOK, rows.shape[-1]), F32)
        for k in FARS:
            if k:
                back(n, k).wait_recv()
            for i in range(2):
                total = total + jnp.dot(comb_ref[k, i], rows[k], preferred_element_type=F32)
        return total

    def token_sum(i):
        to = rem(y + i, NY)
        return send(my_ref.at[to], ly_ref.at[y], ds.at[i], dr.at[i], at(g, z, to, t))

    def part(zi, zo):
        return send(m_ref.at[zo], l_ref.at[zi], cs.at[zo], cr.at[zi], at(g, zo, y, t))

    def home(zo):
        @pl.when(zo != z)
        def _():
            part(z, zo).start()

    def combine(n):
        total = combined(n)
        for i, zo in enumerate(PARTS[n]):
            m_ref[zo] = total[:, i * FEAT:(i + 1) * FEAT].astype(BF)
        for zo in PARTS[n]:
            home(zo)

    lax.fori_loop(0, NT, sweep0, 0)
    lax.fori_loop(0, NT, sweep1, 0)
    total = combined(2)
    for i in range(NY):
        my_ref[i] = total[:, i * FEAT:(i + 1) * FEAT].astype(BF)
    for i in (1, 3, 2):
        token_sum(i).start()
    lax.fori_loop(0, NT, sweep2, 0)
    combine(0)
    ly_ref[y] = my_ref[y]
    for i in (1, 3, 2):
        token_sum(i).wait_recv()
    total = jnp.zeros((TOK, FEAT), F32)
    for i in range(NY):
        total = total + ly_ref[i].astype(F32)
    m_ref[LATE] = total.astype(BF)
    home(LATE)
    lax.fori_loop(0, NT, sweep3, 0)
    combine(1)

    l_ref[z] = m_ref[z]
    own = jnp.zeros((TOK, FEAT), F32)
    for zi in range(NZ):
        @pl.when(zi != z)
        def _():
            part(zi, z).wait_recv()
    for zi in range(NZ):
        own = own + l_ref[zi].astype(F32)
    out_ref[...] = own.astype(BF)

    for m in served:
        m.wait()
    for i in (1, 2, 3):
        tok_copy(i).wait_send()
        tok_along(i).wait_send()
        token_sum(i).wait_send()
    wave_left(2)
    wave_left(3)
    for j in range(NZ):
        for q in range(2):
            if j or q:
                second(j, q).wait_send()
    for k in range(1, NT):
        across(2, k).wait_send()
        back(2, k).wait_send()
    for n in range(2):
        for k in range(NT):
            for way in range(3):
                along(n, k, way).wait_send()
            if k:
                across(n, k).wait_send()
                back(n, k).wait_send()
            far(n, k).wait_send()
            plain(n, k).wait_send()
            summed(n, k).wait_send()
    for zo in range(NZ):
        @pl.when(zo != z)
        def _():
            part(z, zo).wait_send()


def hand_over(*refs):
    src, dst, held, ins, outs = refs[:4], refs[4:8], refs[8:12], refs[12], refs[13]
    reads = [pltpu.make_async_copy(src[i], held[i], ins.at[i]) for i in range(4)]
    writes = [pltpu.make_async_copy(held[i], dst[i], outs.at[i]) for i in range(4)]
    for r in reads:
        r.start()
    for r, w in zip(reads, writes):
        r.wait()
        w.start()
    for w in writes:
        w.wait()


def local(tokens, routes, route_weight, norm_gain, gate_master, up_master, down_master):
    vm = pl.BlockSpec(memory_space=pltpu.VMEM)
    any_ = pl.BlockSpec(memory_space=pl.ANY)
    dma = pltpu.SemaphoreType.DMA
    serving = jax.ShapeDtypeStruct((1, COLS, MODEL), BF)
    mixed = jax.ShapeDtypeStruct((TOK, FEAT), BF)
    master = pltpu.VMEM((EXPERTS, ROWS, WIDTH), F32)

    def rows(*dims):
        return pltpu.VMEM((*dims[:-1], CAP, dims[-1]), BF)

    def summing(width):
        return [rows(NT, NY, width)] + [rows(NT, width)] * 6

    shapes = (mixed, serving, serving, serving)
    results = pl.pallas_call(
        kernel,
        out_shape=shapes,
        in_specs=[vm, vm, vm, vm, any_, any_, any_],
        out_specs=(vm, any_, any_, any_),
        scratch_shapes=[
            master, master, master,
            pltpu.VMEM((16, TOK), F32),
            pltpu.VMEM((16, TOK), F32),
            pltpu.VMEM((NT, CAP, TOK), BF),
            pltpu.VMEM((NT, 2, TOK, CAP), BF),
            pltpu.VMEM((NT, 2, PACK, LANES), BF),
            pltpu.VMEM((NX, NY, PACK, LANES), BF),
            pltpu.VMEM((2 * NZ, NY, PACK, LANES), BF),
            pltpu.VMEM((NZ, TOK, FEAT), BF),
            pltpu.VMEM((NY, TOK, FEAT), BF),
            rows(NT, FEAT), rows(NT, 2, FEAT), rows(NT, NY, FEAT),
            rows(NZ, NT, NY, FEAT),
            pltpu.VMEM((COLS, MODEL), BF),
            pltpu.VMEM((COLS, MODEL), BF),
            pltpu.VMEM((COLS, MODEL), BF),
            rows(NT, COLS),
            *summing(2 * FEAT), *summing(FEAT),
            rows(NT, NY * FEAT), rows(NT, NY * FEAT),
            pltpu.VMEM((NY, TOK, FEAT), BF),
            pltpu.VMEM((NY, TOK, FEAT), BF),
            pltpu.VMEM((NZ, TOK, FEAT), BF),
            pltpu.VMEM((NZ, TOK, FEAT), BF),
            dma((3,)), dma((NZ,)), dma((NZ,)), dma((NY,)), dma((NY,)),
            dma((NT, 2)), dma((NX * NY,)),
            dma((NZ, 2)), dma((NZ, 2)),
            dma((3, NT)), dma((3, NT)),
            dma((2, NT, 3)), dma((2, NT, 3)),
            dma((2, NT)), dma((2, NT)), dma((2, NT)), dma((2, NT)),
            dma((2, NT)), dma((2, NT)), dma((3, NT)), dma((3, NT)),
            dma((NY,)), dma((NY,)),
            dma((NZ,)), dma((NZ,)), dma((3,)),
        ],
        compiler_params=pltpu.CompilerParams(collective_id=0, has_side_effects=True, vmem_limit_bytes=VMEM_LIMIT),
        name="handover_kernel",
    )(tokens, routes.T, route_weight.T, norm_gain[None, :], gate_master, up_master, down_master)
    out, gate_t, up_t, down_t = pl.pallas_call(
        hand_over,
        out_shape=shapes,
        in_specs=[any_] * 4,
        out_specs=(any_,) * 4,
        scratch_shapes=[pltpu.VMEM(v.shape, BF) for v in shapes] + [dma((4,)), dma((4,))],
        name="output_kernel",
    )(*results)
    return out, jnp.swapaxes(gate_t, 1, 2), jnp.swapaxes(up_t, 1, 2), jnp.swapaxes(down_t, 1, 2)


def solution(mesh):
    placed = (
        P(("gr", "tp"), "fs"),
        P(("gr", "tp"), None),
        P(("gr", "tp"), None),
        P(("gr", "fs")),
        P(None, ("gr", "fs"), "tp"),
        P(None, ("gr", "fs"), "tp"),
        P(None, ("gr", "fs"), "tp"),
    )
    return jax.shard_map(
        local,
        mesh=mesh,
        in_specs=placed,
        out_specs=(
            P(("gr", "tp"), "fs"),
            P("tp", None, "fs"),
            P("tp", None, "fs"),
            P("tp", None, "fs"),
        ),
        check_vma=False,
    )
```

```python
import jax
import jax.numpy as jnp
from jax import lax
from jax.experimental import pallas as pl
from jax.experimental.pallas import tpu as pltpu
from jax.sharding import PartitionSpec as P

norm_eps = 1e-06
BF = jnp.bfloat16
F32 = jnp.float32
I32 = jnp.int32
MESH = pl.DeviceIdType.MESH
VMEM_LIMIT = 60 * 1024 * 1024

NY, NZ, NX, NC = 4, 4, 4, 2
NT = NX * NC
EXPERTS = 8
CAP = 192
ROWS = 64
WIDTH = 352
COLS = 176
LANES = 128
DOWN = COLS // 2
PACK = COLS + DOWN
TOK = 512
FEAT = 128
MODEL = 2048
NEAR = (0, 1, 7, 2, 6, 3, 5, 4)
FARS = (4, 3, 5, 2, 6, 1, 7, 0)
PARTS = ((0, 3), (2,))
LATE = 1


def rem(a, n):
    return lax.rem(a, n)


def at(g, z, y, t):
    return (g, z * NY + y, t)


def send(src, dst, ss, rs, to):
    return pltpu.make_async_remote_copy(
        src_ref=src, dst_ref=dst, send_sem=ss, recv_sem=rs, device_id=to, device_id_type=MESH
    )


def kernel(
    tok_ref, routes_ref, weight_ref, gain_ref, gm_hbm, um_hbm, dm_hbm,
    out_ref, gate_out, up_out, down_out,
    gm_ref, um_ref, dm_ref, key_ref, mix_ref, table_ref, comb_ref,
    wp_ref, q_ref, v_ref, t_ref, ty_ref, s0_ref, s1_ref, s2_ref, x_ref, gate_ref, up_ref, down_ref, h_ref,
    p0, r0, a0, u0, w0, o0, e0, p1, r1, a1, u1, w1, o1, e1, pl_ref, el_ref, my_ref, ly_ref, m_ref, l_ref,
    ms, zs, zr, tys, tyr, qs, qr, vs, vr, xs, xr, ys, yr,
    fs, fr, us, ur, ws, wr, bs, br, ds, dr, cs, cr, outs,
):
    ps, rs_, as_, us_, ws_, os_, es = ((p0, p1), (r0, r1), (a0, a1), (u0, u1), (w0, w1), (o0, o1), (e0, e1))
    g, f, t = lax.axis_index("gr"), lax.axis_index("fs"), lax.axis_index("tp")
    z, y = lax.div(f, NY), rem(f, NY)
    x, c = lax.div(t, NC), rem(t, NC)
    up_y, dn_y, far_y = rem(y + 1, NY), rem(y + NY - 1, NY), rem(y + 2, NY)

    masters = [
        pltpu.make_async_copy(src, dst, ms.at[i])
        for i, (src, dst) in enumerate(((gm_hbm, gm_ref), (um_hbm, um_ref), (dm_hbm, dm_ref)))
    ]
    for m in masters:
        m.start()

    barrier = pltpu.get_barrier_semaphore()
    count = 0
    for dy in range(NY):
        for dt in range(NT):
            if dy or dt:
                pl.semaphore_signal(barrier, inc=1, device_id=at(g, z, rem(y + dy, NY), rem(t + dt, NT)), device_id_type=MESH)
                count += 1
    for dg in range(2):
        for dz in range(NZ):
            if dg or dz:
                pl.semaphore_signal(barrier, inc=1, device_id=at(rem(g + dg, 2), rem(z + dz, NZ), y, t), device_id_type=MESH)
                count += 1

    ex = lax.broadcasted_iota(I32, (16, TOK), 0)
    first_is, second_is = routes_ref[0:1, :] == ex, routes_ref[1:2, :] == ex
    named = first_is | second_is
    before = lax.broadcasted_iota(I32, (TOK, TOK), 0) < lax.broadcasted_iota(I32, (TOK, TOK), 1)
    rank = jnp.dot(
        jnp.where(named, 1.0, 0.0).astype(BF), jnp.where(before, 1.0, 0.0).astype(BF), preferred_element_type=F32
    )
    key_ref[...] = jnp.where(named, rank, -1.0)
    mix_ref[...] = jnp.where(first_is, weight_ref[0:1, :], 0.0) + jnp.where(second_is, weight_ref[1:2, :], 0.0)
    slot = lax.broadcasted_iota(I32, (CAP, TOK), 0).astype(F32)

    def tables(k, _):
        key = key_ref[pl.ds(rem(t + k, NT), 1), :]
        table_ref[k] = jnp.where(slot == key, 1.0, 0.0).astype(BF)
        return 0

    lax.fori_loop(0, NT, tables, 0)
    ty_ref[y] = tok_ref[...]

    def weighting(k, _):
        e = rem(t + NT - k, NT)
        here = slot == key_ref[pl.ds(e, 1), :]
        mix = mix_ref[pl.ds(e, 1), :]
        high = mix.astype(BF).astype(F32)
        for i, part in enumerate((high, mix - high)):
            comb_ref[k, i] = jnp.transpose(jnp.where(here, part, 0.0)).astype(BF)
        return 0

    lax.fori_loop(0, NT, weighting, 0)

    for m in masters:
        m.wait()
    gain = jnp.concatenate([gain_ref[...], gain_ref[...]], axis=1)

    def pack(e, _):
        pad = jnp.zeros((2 * ROWS, 3 * LANES - WIDTH), F32)
        gu = jnp.concatenate([gm_ref[e], um_ref[e]], axis=0)
        gu = jnp.transpose(jnp.concatenate([gu, pad], axis=1)) * gain
        dn = dm_ref[e]
        dn = jnp.concatenate([dn, pad[:ROWS]], axis=1)
        dd = jnp.concatenate([dn, pltpu.roll(dn, 3 * LANES - DOWN, 1)], axis=0)
        dd = jnp.transpose(dd)
        for h in range(2):
            lo = h * COLS
            wp_ref[e, h] = jnp.concatenate([gu[lo:lo + COLS], dd[lo:lo + DOWN]], axis=0).astype(BF)

        return 0

    lax.fori_loop(0, NT, pack, 0)
    pl.semaphore_wait(barrier, count)

    low, base = rem(z, 2), 2 * lax.div(z, 2)
    peers = {1: base + 1 - low, 2: 2 - base + low, 3: 3 - base - low}

    def tok_copy(i):
        return send(tok_ref, t_ref.at[z], zs.at[i], zr.at[i], at(g, peers[i], y, t))

    def tok_along(i):
        return send(tok_ref, ty_ref.at[y], tys.at[i], tyr.at[i], at(g, z, rem(y + i, NY), t))

    def first(e, h):
        return send(
            wp_ref.at[e, h], q_ref.at[x, y], qs.at[e, h], qr.at[x * NY + y], at(g, z, NC * c + h, e)
        )

    def stays(e, h):
        return (NC * c + h == y) & (e == t)

    def pieces(i):
        return [(NC * rem(x + 2 * NX - z - i, NX) + n, h) for n in range(NC) for h in range(2)]

    def wave(i):
        for e, h in pieces(i):
            @pl.when(stays(e, h))
            def _():
                pltpu.make_async_copy(wp_ref.at[e, h], q_ref.at[x, y], qr.at[x * NY + y]).start()

            @pl.when(jnp.logical_not(stays(e, h)))
            def _():
                first(e, h).start()

    def wave_left(i):
        for e, h in pieces(i):
            @pl.when(jnp.logical_not(stays(e, h)))
            def _():
                first(e, h).wait_send()

    tok_copy(1).start()
    wave(0)
    wave(1)
    tok_copy(2).start()
    tok_copy(3).start()


    mate, rest = peers[1], 2 - base
    tiles = (mate, pl.ds(rest, 2))
    stage = (s0_ref, s1_ref)

    def dispatch(q):
        rows_in = t_ref[mate] if q == 0 else jnp.concatenate([t_ref[rest], t_ref[rest + 1]], axis=1)
        for k in NEAR:
            rows = jnp.dot(table_ref[k], rows_in, preferred_element_type=F32).astype(BF)
            for i in range(1 + q):
                part = rows[:, i * FEAT:(i + 1) * FEAT]
                if k == 0:
                    x_ref[rest + i if q else mate, t, y] = part
                elif q:
                    s1_ref[k, i] = part
                else:
                    s0_ref[k] = part

    def dispatch_own():
        rows_in = jnp.concatenate([ty_ref[i] for i in range(NY)], axis=1)
        for k in NEAR:
            rows = jnp.dot(table_ref[k], rows_in, preferred_element_type=F32).astype(BF)
            for i in range(NY):
                part = rows[:, i * FEAT:(i + 1) * FEAT]
                if k == 0:
                    x_ref[z, t, i] = part
                else:
                    s2_ref[k, i] = part

    def across(q, k):
        if q == 2:
            src, dst = s2_ref.at[k], x_ref.at[z, t]
        else:
            src, dst = stage[q].at[k], x_ref.at[tiles[q], t, y]
        return send(src, dst, xs.at[q, k], xr.at[q, k], at(g, z, y, rem(t + k, NT)))

    def along(q, k, way):
        b = rem(t + NT - k, NT)
        whose = y if way < 2 else (dn_y if k % 2 == 0 else up_y)
        to = up_y if way == 0 or (way == 2 and k % 2 == 0) else dn_y
        ref = x_ref.at[tiles[q], b, whose]
        return send(ref, ref, ys.at[q, k, way], yr.at[q, k, way], at(g, z, to, t))

    def spread(q, k):
        if k:
            across(q, k).wait_recv()
        along(q, k, 0).start()
        along(q, k, 1).start()

    def forward(q, k):
        along(q, k, k % 2).wait_recv()
        along(q, k, 2).start()

    zz = g * NZ + z

    def second(j, q):
        zd = rem(z + j, NZ)
        return send(q_ref.at[zd], v_ref.at[zz], vs.at[j, q], vr.at[j, q], at(rem(g + q, 2), zd, y, t))

    own_v = pltpu.make_async_copy(q_ref.at[z], v_ref.at[zz], vr.at[0, 0])

    def weights_on(i):
        zd = rem(x + z + i, NX)
        for n in range(NY):
            send(q_ref.at[zd, n], q_ref.at[zd, n], qs.at[0, 0], qr.at[zd * NY + n], at(g, z, up_y, t)).wait_recv()
        j = rem(zd + NZ - z, NZ)
        second(j, 1).start()

        @pl.when(j > 0)
        def _():
            second(j, 0).start()

        @pl.when(j == 0)
        def _():
            own_v.start()

    tok_copy(1).wait_recv()
    wave_left(0)
    wave(2)
    dispatch(0)
    for k in NEAR[1:]:
        across(0, k).start()
    spread(0, 0)
    weights_on(0)
    wave_left(1)
    wave(3)
    for i in (1, 3, 2):
        tok_along(i).start()
    weights_on(1)
    tok_copy(2).wait_recv()
    tok_copy(3).wait_recv()
    dispatch(1)
    for k in NEAR[1:]:
        across(1, k).start()
    spread(1, 0)
    weights_on(2)
    weights_on(3)
    for k in NEAR[1:]:
        spread(0, k)
    for i in (1, 3, 2):
        tok_along(i).wait_recv()
    dispatch_own()
    for k in NEAR:
        forward(0, k)
        if k:
            spread(1, k)
    for k in FARS[:-1]:
        across(2, k).start()
    for k in NEAR:
        forward(1, k)

    left = lax.broadcasted_iota(I32, (COLS, LANES), 1) < ROWS

    def unpack(zs_):
        for i in range(NY // 2):
            a, b = (v_ref[zs_, 2 * i + n].astype(F32) for n in range(2))
            ra, rb = pltpu.roll(a, ROWS, 1), pltpu.roll(b, ROWS, 1)
            cols = pl.ds(pl.multiple_of((zs_ * (NY // 2) + i) * LANES, LANES), LANES)
            gate_ref[:, cols] = jnp.where(left, a[:COLS], rb[:COLS]).astype(BF)
            up_ref[:, cols] = jnp.where(left, ra[:COLS], b[:COLS]).astype(BF)
            down_ref[:, cols] = jnp.concatenate(
                [jnp.where(left[:DOWN], a[COLS:], rb[COLS:]), jnp.where(left[:DOWN], ra[COLS:], b[COLS:])], axis=0
            ).astype(BF)

    own_v.wait()
    unpack(zz)
    for j, q in ((1, 0), (3, 0), (2, 0), (1, 1), (3, 1), (2, 1), (0, 1)):
        second(j, q).wait_recv()
        unpack(rem(g + q, 2) * NZ + rem(z + NZ - j, NZ))
    served = [
        pltpu.make_async_copy(src, dst.at[0], outs.at[i])
        for i, (src, dst) in enumerate(((gate_ref, gate_out), (up_ref, up_out), (down_ref, down_out)))
    ]
    for m in served:
        m.start()

    for q in range(2):
        for k in NEAR:
            along(q, k, 1 - k % 2).wait_recv()
            along(q, k, 2).wait_recv()
    for k in FARS[:-1]:
        across(2, k).wait_recv()

    def near(k):
        return rem(y + 1 + 2 * rem(k, 2), NY)

    def other(k):
        return rem(y + 3 - 2 * rem(k, 2), NY)

    def far(n, k):
        return send(ps[n].at[k, far_y], rs_[n].at[k], fs.at[n, k], fr.at[n, k], at(g, z, near(k), t))

    def plain(n, k):
        return send(ps[n].at[k, other(k)], us_[n].at[k], us.at[n, k], ur.at[n, k], at(g, z, other(k), t))

    def summed(n, k):
        return send(as_[n].at[k], ws_[n].at[k], ws.at[n, k], wr.at[n, k], at(g, z, near(k), t))

    def back(n, k):
        src, dst = (os_[n].at[k], es[n].at[k]) if n < 2 else (pl_ref.at[k], el_ref.at[k])
        return send(src, dst, bs.at[n, k], br.at[n, k], at(g, z, y, rem(t + k, NT)))

    def experts(k):
        b = rem(t + k, NT)
        rows = jnp.concatenate(
            [x_ref[zi, b, yi] for zi in range(NZ) for yi in range(NY)],
            axis=1,
        )
        wide = rows.astype(F32)
        scale = lax.rsqrt(jnp.sum(wide * wide, axis=1, keepdims=True) / MODEL + norm_eps)
        rows = (wide * scale).astype(BF)
        dims = (((1,), (1,)), ((), ()))
        gate = lax.dot_general(rows, gate_ref[...], dims, preferred_element_type=F32)
        up = lax.dot_general(rows, up_ref[...], dims, preferred_element_type=F32)
        h_ref[k] = (gate / (1.0 + jnp.exp(-gate)) * up).astype(BF)

    def product(zi, k):
        cols = slice(zi * NY * FEAT, (zi + 1) * NY * FEAT)
        return jnp.dot(h_ref[k], down_ref[:, cols], preferred_element_type=F32).astype(BF)

    def products(n, k):
        for i, zi in enumerate(PARTS[n]):
            part = product(zi, k)
            for yi in range(NY):
                ps[n][k, yi, :, i * FEAT:(i + 1) * FEAT] = part[:, yi * FEAT:(yi + 1) * FEAT]

    def kth(i):
        return 4 + (1 - 2 * rem(i, 2)) * lax.div(i + 1, 2)

    def sweep0(i, _):
        k = kth(i)
        experts(k)
        products(0, k)
        far(0, k).start()
        plain(0, k).start()
        late = product(LATE, k)

        @pl.when(k > 0)
        def _():
            pl_ref[k] = late
            back(2, k).start()

        @pl.when(k == 0)
        def _():
            el_ref[k] = late

        return 0

    def relay(n, k):
        far(n, k).wait_recv()
        as_[n][k] = (rs_[n][k].astype(F32) + ps[n][k, near(k)].astype(F32)).astype(BF)
        summed(n, k).start()

    def finish(n, k):
        plain(n, k).wait_recv()
        summed(n, k).wait_recv()
        total = (ps[n][k, y].astype(F32) + us_[n][k].astype(F32) + ws_[n][k].astype(F32)).astype(BF)

        @pl.when(k > 0)
        def _():
            os_[n][k] = total
            back(n, k).start()

        @pl.when(k == 0)
        def _():
            es[n][k] = total

    def sweep1(i, _):
        k = kth(i)
        relay(0, k)
        products(1, k)
        far(1, k).start()
        plain(1, k).start()
        return 0

    def sweep2(i, _):
        k = kth(i)
        relay(1, k)
        finish(0, k)
        return 0

    def sweep3(i, _):
        finish(1, kth(i))
        return 0

    def combined(n):
        rows = es[n] if n < 2 else el_ref
        total = jnp.zeros((TOK, rows.shape[-1]), F32)
        for k in FARS:
            if k:
                back(n, k).wait_recv()
            for i in range(2):
                total = total + jnp.dot(comb_ref[k, i], rows[k], preferred_element_type=F32)
        return total

    def token_sum(i):
        to = rem(y + i, NY)
        return send(my_ref.at[to], ly_ref.at[y], ds.at[i], dr.at[i], at(g, z, to, t))

    def part(zi, zo):
        return send(m_ref.at[zo], l_ref.at[zi], cs.at[zo], cr.at[zi], at(g, zo, y, t))

    def home(zo):
        @pl.when(zo != z)
        def _():
            part(z, zo).start()

    def combine(n):
        total = combined(n)
        for i, zo in enumerate(PARTS[n]):
            m_ref[zo] = total[:, i * FEAT:(i + 1) * FEAT].astype(BF)
        for zo in PARTS[n]:
            home(zo)

    lax.fori_loop(0, NT, sweep0, 0)
    lax.fori_loop(0, NT, sweep1, 0)
    total = combined(2)
    for i in range(NY):
        my_ref[i] = total[:, i * FEAT:(i + 1) * FEAT].astype(BF)
    for i in (1, 3, 2):
        token_sum(i).start()
    lax.fori_loop(0, NT, sweep2, 0)
    combine(0)
    ly_ref[y] = my_ref[y]
    for i in (1, 3, 2):
        token_sum(i).wait_recv()
    total = jnp.zeros((TOK, FEAT), F32)
    for i in range(NY):
        total = total + ly_ref[i].astype(F32)
    m_ref[LATE] = total.astype(BF)
    home(LATE)
    lax.fori_loop(0, NT, sweep3, 0)
    combine(1)

    l_ref[z] = m_ref[z]
    own = jnp.zeros((TOK, FEAT), F32)
    for zi in range(NZ):
        @pl.when(zi != z)
        def _():
            part(zi, z).wait_recv()
    for zi in range(NZ):
        own = own + l_ref[zi].astype(F32)
    out_ref[...] = own.astype(BF)

    for m in served:
        m.wait()
    for i in (1, 2, 3):
        tok_copy(i).wait_send()
        tok_along(i).wait_send()
        token_sum(i).wait_send()
    wave_left(2)
    wave_left(3)
    for j in range(NZ):
        for q in range(2):
            if j or q:
                second(j, q).wait_send()
    for k in range(1, NT):
        across(2, k).wait_send()
        back(2, k).wait_send()
    for n in range(2):
        for k in range(NT):
            for way in range(3):
                along(n, k, way).wait_send()
            if k:
                across(n, k).wait_send()
                back(n, k).wait_send()
            far(n, k).wait_send()
            plain(n, k).wait_send()
            summed(n, k).wait_send()
    for zo in range(NZ):
        @pl.when(zo != z)
        def _():
            part(z, zo).wait_send()


def hand_over(*refs):
    src, dst, held, ins, outs = refs[:4], refs[4:8], refs[8:12], refs[12], refs[13]
    reads = [pltpu.make_async_copy(src[i], held[i], ins.at[i]) for i in range(4)]
    writes = [pltpu.make_async_copy(held[i], dst[i], outs.at[i]) for i in range(4)]
    for r in reads:
        r.start()
    for r, w in zip(reads, writes):
        r.wait()
        w.start()
    for w in writes:
        w.wait()


def local(tokens, routes, route_weight, norm_gain, gate_master, up_master, down_master):
    vm = pl.BlockSpec(memory_space=pltpu.VMEM)
    any_ = pl.BlockSpec(memory_space=pl.ANY)
    dma = pltpu.SemaphoreType.DMA
    serving = jax.ShapeDtypeStruct((1, COLS, MODEL), BF)
    mixed = jax.ShapeDtypeStruct((TOK, FEAT), BF)
    master = pltpu.VMEM((EXPERTS, ROWS, WIDTH), F32)

    def rows(*dims):
        return pltpu.VMEM((*dims[:-1], CAP, dims[-1]), BF)

    def summing(width):
        return [rows(NT, NY, width)] + [rows(NT, width)] * 6

    shapes = (mixed, serving, serving, serving)
    results = pl.pallas_call(
        kernel,
        out_shape=shapes,
        in_specs=[vm, vm, vm, vm, any_, any_, any_],
        out_specs=(vm, any_, any_, any_),
        scratch_shapes=[
            master, master, master,
            pltpu.VMEM((16, TOK), F32),
            pltpu.VMEM((16, TOK), F32),
            pltpu.VMEM((NT, CAP, TOK), BF),
            pltpu.VMEM((NT, 2, TOK, CAP), BF),
            pltpu.VMEM((NT, 2, PACK, LANES), BF),
            pltpu.VMEM((NX, NY, PACK, LANES), BF),
            pltpu.VMEM((2 * NZ, NY, PACK, LANES), BF),
            pltpu.VMEM((NZ, TOK, FEAT), BF),
            pltpu.VMEM((NY, TOK, FEAT), BF),
            rows(NT, FEAT), rows(NT, 2, FEAT), rows(NT, NY, FEAT),
            rows(NZ, NT, NY, FEAT),
            pltpu.VMEM((COLS, MODEL), BF),
            pltpu.VMEM((COLS, MODEL), BF),
            pltpu.VMEM((COLS, MODEL), BF),
            rows(NT, COLS),
            *summing(2 * FEAT), *summing(FEAT),
            rows(NT, NY * FEAT), rows(NT, NY * FEAT),
            pltpu.VMEM((NY, TOK, FEAT), BF),
            pltpu.VMEM((NY, TOK, FEAT), BF),
            pltpu.VMEM((NZ, TOK, FEAT), BF),
            pltpu.VMEM((NZ, TOK, FEAT), BF),
            dma((3,)), dma((NZ,)), dma((NZ,)), dma((NY,)), dma((NY,)),
            dma((NT, 2)), dma((NX * NY,)),
            dma((NZ, 2)), dma((NZ, 2)),
            dma((3, NT)), dma((3, NT)),
            dma((2, NT, 3)), dma((2, NT, 3)),
            dma((2, NT)), dma((2, NT)), dma((2, NT)), dma((2, NT)),
            dma((2, NT)), dma((2, NT)), dma((3, NT)), dma((3, NT)),
            dma((NY,)), dma((NY,)),
            dma((NZ,)), dma((NZ,)), dma((3,)),
        ],
        compiler_params=pltpu.CompilerParams(collective_id=0, has_side_effects=True, vmem_limit_bytes=VMEM_LIMIT),
        name="handover_kernel",
    )(tokens, routes.T, route_weight.T, norm_gain[None, :], gate_master, up_master, down_master)
    out, gate_t, up_t, down_t = pl.pallas_call(
        hand_over,
        out_shape=shapes,
        in_specs=[any_] * 4,
        out_specs=(any_,) * 4,
        scratch_shapes=[pltpu.VMEM(v.shape, BF) for v in shapes] + [dma((4,)), dma((4,))],
        name="output_kernel",
    )(*results)
    return out, jnp.swapaxes(gate_t, 1, 2), jnp.swapaxes(up_t, 1, 2), jnp.swapaxes(down_t, 1, 2)


def solution(mesh):
    placed = (
        P(("gr", "tp"), "fs"),
        P(("gr", "tp"), None),
        P(("gr", "tp"), None),
        P(("gr", "fs")),
        P(None, ("gr", "fs"), "tp"),
        P(None, ("gr", "fs"), "tp"),
        P(None, ("gr", "fs"), "tp"),
    )
    return jax.shard_map(
        local,
        mesh=mesh,
        in_specs=placed,
        out_specs=(
            P(("gr", "tp"), "fs"),
            P("tp", None, "fs"),
            P("tp", None, "fs"),
            P("tp", None, "fs"),
        ),
        check_vma=False,
    )
```
